256 devices in a mesh: sp: 64 (over z, x, core), tp: 4 (over y).
Axes of the slice: x: 4, y: 4, z: 8, core: 2. Of those that a mesh axis runs over, the one named last changes fastest.
Arguments:
- stream_in: bfloat16 [16384, 2048], P(('sp', 'tp')), may hold values from -6 to 6
- queries: bfloat16 [16384, 1024], P('sp', 'tp'), may hold values from -48 to 48
- keys: bfloat16 [16384, 512], P('sp', 'tp'), may hold values from -48 to 48
- values: bfloat16 [16384, 512], P('sp', 'tp'), may hold values from -6 to 6
- query_gain: float32 [64], replicated, may hold values from 1.5 to 6
- key_gain: float32 [64], replicated, may hold values from 1.5 to 6
- out_rows: bfloat16 [1024, 2048], P('tp'), may hold values from -0.1875 to 0.1875
- norm_gain: float32 [2048], replicated, may hold values from 0.1 to 1.9
- route_ids: int32 [16384, 2], P(('sp', 'tp')), may hold values from 0 to 63, all different within a row; in each aligned block of 64 rows (0 to 63, 64 to 127, ...) at most 3 rows name the same one
- route_weights: float32 [16384, 2], P(('sp', 'tp')), may hold values from 0.25 to 1
- gate_weight: bfloat16 [64, 2048, 3072], P('sp', None, 'tp'), may hold values from -0.125 to 0.125
- up_weight: bfloat16 [64, 2048, 3072], P('sp', None, 'tp'), may hold values from -0.125 to 0.125
- down_weight: bfloat16 [64, 3072, 2048], P('sp', 'tp'), may hold values from -0.109375 to 0.109375
Outputs:
- stream_out: bfloat16 [16384, 2048], P(('sp', 'tp'))
The draws below stay inside these ranges and needn't reach their ends.
Inputs may be any that keep to these rules, and one draw needn't show every extreme that they name: `route_ids`: each row names 2 different experts; among the rows of one device no expert is named more than 3 times.
All inputs are finite; a program needn't handle non-finite values.
Results may differ from the reference program's by a relative error of at most 0.014.
The reference program's roundings to bfloat16 on the way count: a program that leaves them out, or rounds other values in their place, can miss the bound.
Values may be sent and summed in bfloat16 or wider, within the bound.
A program may use at most 128 MiB of HBM per device.

```python
import math
import jax
import jax.numpy as jnp
import numpy as np
from jax import lax

D = 2048
QUERY_HEAD_COUNT = 16
KEY_VALUE_HEADS = 8
HEAD_DIMENSION = 64
FF = 3072
TOPK = 2
GRID_W = 64
SEQ_LEN = 16384
TOTAL_TOKENS = 16384
TL = 64
ATTN_W = 1024
EXPERTS = 64
CAP = 3
N_SP = 64
N_TP = 4


def unrotated_rows(key, width):
    unrotated = jnp.clip(jax.random.normal(key, (TOTAL_TOKENS, width), jnp.float32), -6.0, 6.0)
    return unrotated


def draw_queries(key, part):
    unrotated = unrotated_rows(jax.random.fold_in(key, 11), QUERY_HEAD_COUNT * HEAD_DIMENSION)
    return unrotated.astype(jnp.bfloat16)


def draw_keys(key, part):
    unrotated = unrotated_rows(jax.random.fold_in(key, 21), KEY_VALUE_HEADS * HEAD_DIMENSION)
    return unrotated.astype(jnp.bfloat16)


def gain_table(key):
    spread = jax.random.uniform(key, (HEAD_DIMENSION,), jnp.float32, 1.5, 2.5)
    return spread


def draw_query_gain(key, part):
    return gain_table(jax.random.fold_in(key, 31))


def draw_key_gain(key, part):
    return gain_table(jax.random.fold_in(key, 37))


def block_levels(key, dims, shards, smallest, top_value):
    level, own = 1.0, jax.random.fold_in(key, 6)
    for dim, blocks in shards:
        steps = jnp.exp(jax.random.uniform(jax.random.fold_in(own, dim), (blocks,), jnp.float32, smallest / len(shards), top_value / len(shards)))
        level = level * jnp.repeat(steps, dims[dim] // blocks).reshape([-1 if axis == dim else 1 for axis in range(len(dims))])
    return level


def routed_block(rng, own, number, rows, amount, top, limit, lean):
    order = jax.random.permutation(rng, amount)
    crowded, ordinary = portions_of(amount, rows * top, limit, lean, True), portions_of(amount, rows * top, limit, lean, False)
    places = jnp.arange(amount)

    def named(tallies, turn):
        used = int((tallies > 0).sum())
        fixed = max(1, used // 4)
        passed = fixed + (places - fixed + turn * (used - fixed)) % max(1, amount - fixed)
        return jnp.zeros((amount,), jnp.int32).at[order[jnp.where(places < fixed, places, passed)]].set(jnp.asarray(tallies, jnp.int32))

    tallies = jnp.where(number % 4 == 0, named(crowded, number // 4), named(ordinary, number - number // 4 - 1))
    mixed = jax.random.permutation(jax.random.fold_in(own, 3), amount)
    donor, receiver = mixed[0:amount // 2 * 2:2], mixed[1:amount // 2 * 2:2]
    slack = jnp.minimum(tallies[donor] - 1, limit - tallies[receiver]) // 2
    slack = jnp.where((donor == order[0]) | (receiver == order[0]) | (tallies[receiver] == 0), 0, jnp.maximum(slack, 0))
    passed = jax.random.randint(jax.random.fold_in(own, 4), (amount // 2,), 0, 1 << 20) % (slack + 1)
    tallies = tallies.at[donor].add(-passed).at[receiver].add(passed)
    labels = jnp.searchsorted(jnp.cumsum(tallies), jnp.arange(rows * top), side="right").astype(jnp.int32)
    listing = labels.reshape(top, rows).T
    listing = listing[jax.random.permutation(jax.random.fold_in(own, 1), rows)]
    turn = jax.random.randint(jax.random.fold_in(own, 2), (rows, 1), 0, top)
    return jnp.take_along_axis(listing, (jnp.arange(top)[None, :] + turn) % top, axis=1)


def portions_of(amount, total, limit, lean, full):
    portions = [(1 << 20) // math.isqrt(grade ** lean) + 1 for grade in range(1, amount + 1)]
    largest = limit if full else min(limit, max(-(-total // amount), total * portions[0] // sum(portions)))
    least = 1 if total - largest >= amount - 1 else 0
    given, surplus = [largest] + [least] * (amount - 1), total - largest - least * (amount - 1)
    while surplus > 0:
        free = [i for i in range(1, amount) if given[i] < largest] or [i for i in range(1, amount) if given[i] < limit]
        mass, remaining = sum([portions[i] for i in free]), surplus
        for i in free:
            more = min(limit - given[i], max(1, remaining * portions[i] // mass), surplus)
            given[i] = given[i] + more
            surplus = surplus - more
    return np.array(given)


def noise(stream_key, dims, scale, bound, pieces=(), kind=jnp.bfloat16):
    values = scale * jax.random.normal(stream_key, dims, jnp.float32)
    if pieces:
        values = values * block_levels(stream_key, dims, pieces, -0.22, 0.18)
    return jnp.clip(values, -bound, bound).astype(kind)


def setup_inputs(seed: int = 0) -> dict:
    seeds = jax.random.split(jax.random.key(seed), 14)
    stream_in = noise(seeds[0], (TOTAL_TOKENS, D), 1.0, 6.0, ((0, 256),))
    queries = draw_queries(jax.random.fold_in(seeds[13], 71), 0)
    keys = draw_keys(jax.random.fold_in(seeds[13], 71), 0)
    values = noise(seeds[3], (TOTAL_TOKENS, KEY_VALUE_HEADS * HEAD_DIMENSION), 1.0, 6.0, ((0, 64), (1, 4)))
    query_gain = draw_query_gain(jax.random.fold_in(seeds[13], 71), 0)
    key_gain = draw_key_gain(jax.random.fold_in(seeds[13], 71), 0)
    out_rows = noise(seeds[6], (ATTN_W, D), ATTN_W ** -0.5, 0.1875, ((0, 4),))
    norm_gain = jnp.clip(1.0 + 0.18 * jax.random.normal(seeds[7], (D,), jnp.float32), 0.1, 1.9)
    route_ids_keys = jax.random.split(jax.random.fold_in(seeds[8], 1), TOTAL_TOKENS // TL)
    route_ids_turns = jax.random.permutation(jax.random.fold_in(seeds[8], 3), TOTAL_TOKENS // TL)
    route_ids = jax.vmap(lambda own, number: routed_block(jax.random.fold_in(seeds[8], 2), own, number, TL, EXPERTS, TOPK, CAP, 2))(route_ids_keys, route_ids_turns).reshape((TOTAL_TOKENS, TOPK))
    route_weights = jnp.clip(0.25 + 0.75 * jax.random.uniform(seeds[9], (TOTAL_TOKENS, TOPK), jnp.float32) ** block_levels(seeds[9], (TOTAL_TOKENS, TOPK), ((0, 256),), -0.2, 0.2), 0.25, 1.0)
    gate_weight = noise(seeds[10], (EXPERTS, D, FF), D ** -0.5, 0.125, ((0, 64), (2, 4)))
    up_weight = noise(seeds[11], (EXPERTS, D, FF), D ** -0.5, 0.125, ((0, 64), (2, 4)))
    down_weight = noise(seeds[12], (EXPERTS, FF, D), FF ** -0.5, 0.109375, ((0, 64), (1, 4)))
    return {"stream_in": stream_in, "queries": queries, "keys": keys, "values": values, "query_gain": query_gain, "key_gain": key_gain, "out_rows": out_rows, "norm_gain": norm_gain, "route_ids": route_ids, "route_weights": route_weights, "gate_weight": gate_weight, "up_weight": up_weight, "down_weight": down_weight}


EPS = 1e-06
THETA = 10000.0

def turn_tables(offset, count, head_size):
    position = offset + jnp.arange(count, dtype=jnp.int32)
    grid_row = (position // GRID_W).astype(jnp.float32)
    column = (position % GRID_W).astype(jnp.float32)
    pair_index = jnp.arange(head_size // 4, dtype=jnp.float32)
    inverse = THETA ** (-4.0 * pair_index / head_size)
    angles = jnp.concatenate([grid_row[:, None] * inverse, column[:, None] * inverse], axis=1)
    return (jnp.cos(angles), jnp.sin(angles))

def normalize_rotate(block_data, gain_vector, cos_table, sin_table):
    row_count = block_data.shape[0]
    head_size = gain_vector.shape[0]
    wide = block_data.astype(jnp.float32).reshape(row_count, -1, head_size)
    wide = wide * lax.rsqrt(lax.optimization_barrier(jnp.mean(wide * wide, axis=-1, keepdims=True)) + EPS) * gain_vector
    pairs = wide.reshape(row_count, wide.shape[1], head_size // 2, 2)
    even_part = pairs[..., 0]
    odd_part = pairs[..., 1]
    cosine = cos_table[:, None, :]
    sine_part = sin_table[:, None, :]
    turned = jnp.stack([even_part * cosine - odd_part * sine_part, even_part * sine_part + odd_part * cosine], axis=-1)
    return turned.reshape(row_count, -1).astype(jnp.bfloat16)

def attend(rotated_queries, rotated_keys, values):
    sequence_length = rotated_queries.shape[0]
    group_head_count = QUERY_HEAD_COUNT // KEY_VALUE_HEADS
    rows_per_block = math.gcd(sequence_length, 128)
    blocked_queries = rotated_queries.reshape(sequence_length // rows_per_block, rows_per_block, KEY_VALUE_HEADS, group_head_count, HEAD_DIMENSION).astype(jnp.float32)
    every_key_row = rotated_keys.reshape(sequence_length, KEY_VALUE_HEADS, HEAD_DIMENSION).astype(jnp.float32)
    every_value_row = values.reshape(sequence_length, KEY_VALUE_HEADS, HEAD_DIMENSION).astype(jnp.float32)

    def one_block(query_block):
        scores = jnp.einsum('qkgd,skd->qkgs', query_block, every_key_row) * HEAD_DIMENSION ** (-0.5)
        row_top = lax.optimization_barrier(jnp.max(scores, axis=-1, keepdims=True))
        weights = jnp.exp(scores - row_top)
        row_total = lax.optimization_barrier(jnp.sum(weights, axis=-1))
        probs = lax.optimization_barrier(weights.astype(jnp.bfloat16)).astype(jnp.float32)
        mixed_rows = jnp.einsum('qkgs,skd->qkgd', probs, every_value_row) / row_total[..., None]
        return mixed_rows.astype(jnp.bfloat16).reshape(rows_per_block, QUERY_HEAD_COUNT * HEAD_DIMENSION)
    return lax.map(one_block, blocked_queries).reshape(sequence_length, QUERY_HEAD_COUNT * HEAD_DIMENSION)

def reference(stream_in, queries, keys, values, query_gain, key_gain, out_rows, norm_gain, route_ids, route_weights, gate_weight, up_weight, down_weight):
    sequence_length = queries.shape[0]
    sequence_count = sequence_length // SEQ_LEN
    cos_one, sin_one = turn_tables(0, SEQ_LEN, HEAD_DIMENSION)
    cos_table = jnp.tile(cos_one, (sequence_count, 1))
    sin_table = jnp.tile(sin_one, (sequence_count, 1))
    rotated_queries = normalize_rotate(queries, query_gain, cos_table, sin_table)
    rotated_keys = normalize_rotate(keys, key_gain, cos_table, sin_table)

    def one_sequence(triple):
        return attend(triple[0], triple[1], triple[2])
    attended = lax.map(one_sequence, (rotated_queries.reshape(sequence_count, SEQ_LEN, -1), rotated_keys.reshape(sequence_count, SEQ_LEN, -1), values.reshape(sequence_count, SEQ_LEN, -1)))
    attended = attended.reshape(sequence_length, QUERY_HEAD_COUNT * HEAD_DIMENSION)
    projected = jnp.dot(attended, out_rows, preferred_element_type=jnp.float32)
    stream = (stream_in.astype(jnp.float32) + projected).astype(jnp.bfloat16)
    stream_wide = stream.astype(jnp.float32)
    normed = (stream_wide * lax.rsqrt(lax.optimization_barrier(jnp.mean(stream_wide * stream_wide, axis=1, keepdims=True)) + EPS) * norm_gain).astype(jnp.bfloat16)
    flat_ids = route_ids.reshape(-1).astype(jnp.int32)
    total_routes = flat_ids.shape[0]
    most_rows = N_SP * N_TP * CAP
    ordering = jnp.argsort(flat_ids, stable=True).astype(jnp.int32)
    counts = lax.optimization_barrier(jnp.sum((flat_ids[:, None] == jnp.arange(EXPERTS, dtype=jnp.int32)[None, :]).astype(jnp.int32), axis=0)).astype(jnp.int32)
    starts = (jnp.cumsum(counts) - counts).astype(jnp.int32)
    padded = jnp.concatenate([ordering, jnp.zeros((most_rows,), jnp.int32)])
    group_width = FF // N_TP

    def for_expert(results, expert):
        begin = starts[expert].astype(jnp.int32)
        chosen = lax.dynamic_slice(padded, (begin,), (most_rows,))
        valid = jnp.arange(most_rows, dtype=jnp.int32) < counts[expert]
        rows = normed[chosen // TOPK]
        gate_value = jnp.dot(rows, gate_weight[expert], preferred_element_type=jnp.float32)
        up_value = jnp.dot(rows, up_weight[expert], preferred_element_type=jnp.float32)
        hidden = (jax.nn.silu(gate_value) * up_value).astype(jnp.bfloat16)
        partials = jnp.einsum('rgf,gfd->rgd', hidden.reshape(most_rows, N_TP, group_width).astype(jnp.float32), down_weight[expert].reshape(N_TP, group_width, D).astype(jnp.float32))
        partials = lax.optimization_barrier(partials.astype(jnp.bfloat16)).astype(jnp.float32)
        answer = lax.optimization_barrier(jnp.sum(partials, axis=1)).astype(jnp.bfloat16)
        slot_index = jnp.where(valid, chosen, total_routes)
        return (results.at[slot_index].set(answer, mode='drop'), None)
    results = jnp.zeros((total_routes, D), jnp.bfloat16)
    results = lax.scan(for_expert, results, jnp.arange(EXPERTS, dtype=jnp.int32))[0]
    picked = results.reshape(sequence_length, TOPK, D).astype(jnp.float32)
    mixed_out = stream_wide + lax.optimization_barrier(jnp.sum(route_weights[:, :, None] * picked, axis=1))
    return mixed_out.astype(jnp.bfloat16)
```

```python
import jax
import jax.numpy as jnp
from jax import lax
from jax.experimental import pallas as pl
from jax.experimental.pallas import tpu as pltpu
from jax.sharding import PartitionSpec as P

GRID_W = 64
EPS = 1e-06
THETA = 10000.0
NZ, NX = 8, 4
CHIPS = NZ * NX
CHUNK = 2
HALF = 128


def turn_tables(offset, count, head_size):
    position = offset + jnp.arange(count, dtype=jnp.int32)
    grid_row = (position // GRID_W).astype(jnp.float32)
    column = (position % GRID_W).astype(jnp.float32)
    pair_index = jnp.arange(head_size // 4, dtype=jnp.float32)
    inverse = THETA ** (-4.0 * pair_index / head_size)
    lane = jnp.arange(2 * head_size, dtype=jnp.int32) % head_size
    pair = lane // 2
    wide_inverse = jnp.tile(jnp.repeat(inverse, 2), 4)
    place = jnp.where((pair < head_size // 4)[None, :], grid_row[:, None], column[:, None])
    angles = place * wide_inverse
    sign = jnp.where(lane % 2 == 1, 1.0, -1.0)
    return jnp.cos(angles), jnp.sin(angles) * sign


def normalize_turn(x, gain, cosine, sine):
    lane = lax.broadcasted_iota(jnp.int32, x.shape, 1)
    low = lane < 64
    squares = x * x
    first = jnp.sum(jnp.where(low, squares, 0.0), axis=1, keepdims=True)
    second = jnp.sum(jnp.where(low, 0.0, squares), axis=1, keepdims=True)
    mean = jnp.where(low, first, second) * (1.0 / 64)
    wide = x * lax.rsqrt(mean + EPS) * gain
    other = jnp.where(lane % 2 == 1, pltpu.roll(wide, 1, 1), pltpu.roll(wide, 127, 1))
    return wide * cosine + other * sine


def attention_kernel(
    q_ref, k_ref, v_ref, qg_ref, kg_ref, cos_ref, sin_ref, o_ref,
    kv, qz, top, total, acc, send_sem, recv_sem,
):
    me = lax.axis_index("sp")
    core = me % 2
    x = (me // 2) % NX
    z = me // (2 * NX)

    def slot_of(zz, xx, cc):
        return ((zz % NZ) * NX + xx % NX) * 2 + cc

    partner = slot_of(z, x, 1 - core)
    x_up, x_down = slot_of(z, x + 1, core), slot_of(z, x + NX - 1, core)
    z_up, z_down = slot_of(z + 1, x, core), slot_of(z + NZ - 1, x, core)

    barrier = pltpu.get_barrier_semaphore()
    for there in (partner, x_up, x_down, z_up, z_down):
        pl.semaphore_signal(
            barrier, inc=1, device_id={"sp": there}, device_id_type=pl.DeviceIdType.MESH
        )

    cosine, sine = cos_ref[...], sin_ref[...]
    turned = normalize_turn(k_ref[...].astype(jnp.float32), kg_ref[...], cosine, sine).astype(
        jnp.bfloat16
    )
    values_t = v_ref[...].astype(jnp.float32).T.astype(jnp.bfloat16)
    for i in range(2):
        kv[me, i, 0:HALF, :] = turned[i * HALF : (i + 1) * HALF]
        kv[me, i, HALF : 2 * HALF, :] = values_t[:, i * HALF : (i + 1) * HALF]
    pl.semaphore_wait(barrier, 5)

    def copy(slot, half, there):
        return pltpu.make_async_remote_copy(
            src_ref=kv.at[slot, half],
            dst_ref=kv.at[slot, half],
            send_sem=send_sem.at[half],
            recv_sem=recv_sem.at[slot, half],
            device_id={"sp": there},
            device_id_type=pl.DeviceIdType.MESH,
        )

    def arrived(slot, half):
        copy(slot, half, partner).wait_recv()

    def steps(n):
        kz, kx = n // NX, n % NX
        zz = z + NZ + (1 - 2 * (kz % 2)) * ((kz + 1) // 2)
        xx = x + NX + (1 - 2 * (kx % 2)) * ((kx + 1) // 2)
        return kz, kx, zz, xx

    def move(n):
        kz, kx, zz, xx = steps(n)
        slot = slot_of(zz, xx, core)

        @pl.when(n > 0)
        def _():
            arrived(slot, 0)
            arrived(slot, 1)

        z_plus = (kz == 0) | ((kz % 2 == 1) & (kz < 5)) | ((kz == 5) & (core == 0))
        z_minus = (kz == 0) | ((kz % 2 == 0) & (kz < 6)) | ((kz == 6) & (core == 1))
        x_plus = (kx == 0) | ((kx == 1) & (core == 0))
        x_minus = (kx == 0) | ((kx == 2) & (core == 1))

        @pl.when((kx == 0) & z_plus)
        def _():
            copy(slot, 1, z_up).start()

        @pl.when((kx == 0) & z_minus)
        def _():
            copy(slot, 1, z_down).start()

        @pl.when((kz == 0) & x_plus)
        def _():
            copy(slot, 0, x_up).start()

        @pl.when((kz == 0) & x_minus)
        def _():
            copy(slot, 0, x_down).start()

        @pl.when(z_plus)
        def _():
            copy(slot, 0, z_up).start()

        @pl.when(z_minus)
        def _():
            copy(slot, 0, z_down).start()

        @pl.when(x_plus)
        def _():
            copy(slot, 1, x_up).start()

        @pl.when(x_minus)
        def _():
            copy(slot, 1, x_down).start()

        copy(slot, 0, partner).start()
        copy(slot, 1, partner).start()

    move(0)

    for h in range(2):
        part = q_ref[:, h * 128 : (h + 1) * 128].astype(jnp.float32)
        rows = normalize_turn(part, qg_ref[...], cosine, sine).astype(jnp.bfloat16)
        across = (rows.astype(jnp.float32).T * 0.125).astype(jnp.bfloat16)
        qz[h, h * 64 : (h + 1) * 64, 0:256] = across[0:64]
        qz[h, h * 64 : (h + 1) * 64, 256:512] = across[64:128]
        qz[h, (1 - h) * 64 : (2 - h) * 64, :] = jnp.zeros((64, 512), jnp.bfloat16)
    top[...] = jnp.full(top.shape, -1e30, jnp.float32)
    total[...] = jnp.zeros(total.shape, jnp.float32)
    acc[...] = jnp.zeros(acc.shape, jnp.float32)

    for n in range(1, CHUNK):
        move(n)

    def body(step, carry):
        @pl.when(step + 1 < CHIPS // CHUNK)
        def _():
            for i in range(CHUNK):
                move((step + 1) * CHUNK + i)

        blocks = []
        for i in range(CHUNK):
            _, _, zz, xx = steps(step * CHUNK + i)
            theirs = slot_of(zz, xx, 1 - core)
            arrived(theirs, 0)
            arrived(theirs, 1)
            first = slot_of(zz, xx, 0)
            blocks += [kv.at[first + c, j] for c in range(2) for j in range(2)]
        keys = jnp.concatenate([b[0:HALF, :] for b in blocks], axis=0)
        scores = [jnp.dot(keys, qz[h], preferred_element_type=jnp.float32) for h in range(2)]
        for h in range(2):
            old = top[h]
            new = jnp.maximum(old, jnp.max(scores[h], axis=0, keepdims=True))
            weights = jnp.exp(scores[h] - new)
            shrink = jnp.exp(old - new)
            top[h] = new
            total[h] = total[h] * shrink + jnp.sum(weights, axis=0, keepdims=True)
            vt = jnp.concatenate(
                [b[HALF + h * 64 : HALF + (h + 1) * 64, :] for b in blocks], axis=1
            )
            acc[h] = acc[h] * shrink + jnp.dot(
                vt, weights.astype(jnp.bfloat16), preferred_element_type=jnp.float32
            )
        return carry

    lax.fori_loop(0, CHIPS // CHUNK, body, 0)
    parts = []
    for h in range(2):
        mixed = acc[h] / total[h]
        parts += [mixed[:, 0:256], mixed[:, 256:512]]
    o_ref[...] = jnp.concatenate(parts, axis=0).T.astype(jnp.bfloat16)
    for half in range(2):
        everything = kv.at[pl.ds(0, 63), half]
        pltpu.make_async_copy(everything, everything, send_sem.at[half]).wait()


def attention(queries, keys, values, query_gain, key_gain, cosine, sine):
    vmem = pl.BlockSpec(memory_space=pltpu.VMEM)
    return pl.pallas_call(
        attention_kernel,
        out_shape=jax.ShapeDtypeStruct((256, 256), jnp.bfloat16),
        in_specs=[vmem] * 7,
        out_specs=vmem,
        scratch_shapes=[
            pltpu.VMEM((2 * CHIPS, 2, 2 * HALF, 128), jnp.bfloat16),
            pltpu.VMEM((2, 128, 512), jnp.bfloat16),
            pltpu.VMEM((2, 1, 512), jnp.float32),
            pltpu.VMEM((2, 1, 512), jnp.float32),
            pltpu.VMEM((2, 64, 512), jnp.float32),
            pltpu.SemaphoreType.DMA((2,)),
            pltpu.SemaphoreType.DMA((2 * CHIPS, 2)),
        ],
        compiler_params=pltpu.CompilerParams(
            collective_id=0, has_side_effects=True, vmem_limit_bytes=40 * 2**20
        ),
        cost_estimate=pl.CostEstimate(
            flops=8 * 10**9, bytes_accessed=2**20, transcendentals=2**24
        ),
        name="attention",
    )(queries, keys, values, query_gain, key_gain, cosine, sine)


def local(
    stream_in, queries, keys, values, query_gain, key_gain, out_rows, norm_gain,
    route_ids, route_weights, gate_weight, up_weight, down_weight,
):
    head_size = query_gain.shape[0]
    seq_rows = queries.shape[0]
    whole_out = lax.all_gather(out_rows, "tp", axis=0, tiled=True)
    cosine, sine = turn_tables(lax.axis_index("sp") * seq_rows, seq_rows, head_size)
    twice = lambda g: jnp.tile(g, 2)[None, :]
    attended = attention(
        queries, keys, values, twice(query_gain), twice(key_gain), cosine, sine
    )
    token_heads = lax.all_to_all(attended, "tp", split_axis=0, concat_axis=1, tiled=True)
    projected = jnp.dot(token_heads, whole_out, preferred_element_type=jnp.float32)
    stream = (stream_in.astype(jnp.float32) + projected).astype(jnp.bfloat16)
    stream_wide = stream.astype(jnp.float32)
    normed = (
        stream_wide
        * lax.rsqrt(jnp.mean(stream_wide * stream_wide, axis=1, keepdims=True) + EPS)
        * norm_gain
    ).astype(jnp.bfloat16)
    tokens = stream.shape[0]
    model_width = stream.shape[1]
    top_count = route_ids.shape[1]
    experts = lax.axis_size("sp")
    routed = tokens * top_count
    capacity = 3
    flat_ids = route_ids.reshape(routed)
    member = (flat_ids[:, None] == jnp.arange(experts, dtype=jnp.int32)[None, :]).astype(jnp.int32)
    earlier = jnp.cumsum(member, axis=0) - member
    slot_rank = jnp.sum(earlier * member, axis=1)
    target = flat_ids * capacity + slot_rank
    placed = (target[:, None] == jnp.arange(experts * capacity, dtype=jnp.int32)[None, :]).astype(
        jnp.bfloat16
    )
    placed = placed.reshape(tokens, top_count, experts * capacity)
    outgoing = jnp.einsum("tks,td->sd", placed, normed, preferred_element_type=jnp.float32).astype(
        jnp.bfloat16
    )
    outgoing = outgoing.reshape(experts, capacity, model_width)
    arrived = lax.all_to_all(outgoing, "sp", split_axis=0, concat_axis=0, tiled=True)
    flat_rows = arrived.reshape(experts * capacity, model_width)
    row_piece = lax.all_gather(flat_rows, "tp", axis=0, tiled=True)
    gate_value = jnp.dot(row_piece, gate_weight[0], preferred_element_type=jnp.float32)
    up_value = jnp.dot(row_piece, up_weight[0], preferred_element_type=jnp.float32)
    hidden = (jax.nn.silu(gate_value) * up_value).astype(jnp.bfloat16)
    summed = lax.psum_scatter(
        jnp.dot(hidden, down_weight[0], preferred_element_type=jnp.float32).astype(jnp.bfloat16),
        "tp",
        scatter_dimension=0,
        tiled=True,
    )
    answer = summed.reshape(experts, capacity, model_width)
    returned = lax.all_to_all(answer, "sp", split_axis=0, concat_axis=0, tiled=True)
    expert_back = returned.reshape(experts * capacity, model_width)
    picked = jnp.einsum("tks,sd->tkd", placed, expert_back, preferred_element_type=jnp.float32)
    mixed_out = stream_wide + jnp.sum(route_weights[:, :, None] * picked, axis=1)
    return mixed_out.astype(jnp.bfloat16)


def solution(mesh):
    return jax.shard_map(
        local,
        mesh=mesh,
        in_specs=(
            P(("sp", "tp"), None),
            P("sp", "tp"),
            P("sp", "tp"),
            P("sp", "tp"),
            P(),
            P(),
            P("tp", None),
            P(),
            P(("sp", "tp"), None),
            P(("sp", "tp"), None),
            P("sp", None, "tp"),
            P("sp", None, "tp"),
            P("sp", "tp", None),
        ),
        out_specs=P(("sp", "tp"), None),
        check_vma=False,
    )
```

```python
import jax
import jax.numpy as jnp
from jax import lax
from jax.experimental import pallas as pl
from jax.experimental.pallas import tpu as pltpu
from jax.sharding import PartitionSpec as P

GRID_W = 64
EPS = 1e-06
THETA = 10000.0
NZ, NX, NY = 8, 4, 4
CHIPS = NZ * NX
CHUNK = 1
AHEAD = 3
WEIGHTS_AT = 16
SLOTS = 3
HALF = 128


def turn_tables(offset, count, head_size):
    position = offset + jnp.arange(count, dtype=jnp.int32)
    grid_row = (position // GRID_W).astype(jnp.float32)
    column = (position % GRID_W).astype(jnp.float32)
    pair_index = jnp.arange(head_size // 4, dtype=jnp.float32)
    inverse = THETA ** (-4.0 * pair_index / head_size)
    lane = jnp.arange(2 * head_size, dtype=jnp.int32) % head_size
    pair = lane // 2
    wide_inverse = jnp.tile(jnp.repeat(inverse, 2), 4)
    place = jnp.where((pair < head_size // 4)[None, :], grid_row[:, None], column[:, None])
    angles = place * wide_inverse
    sign = jnp.where(lane % 2 == 1, 1.0, -1.0)
    return jnp.cos(angles), jnp.sin(angles) * sign


def normalize_turn(x, gain, cosine, sine):
    lane = lax.broadcasted_iota(jnp.int32, x.shape, 1)
    low = lane < 64
    squares = x * x
    first = jnp.sum(jnp.where(low, squares, 0.0), axis=1, keepdims=True)
    second = jnp.sum(jnp.where(low, 0.0, squares), axis=1, keepdims=True)
    mean = jnp.where(low, first, second) * (1.0 / 64)
    wide = x * lax.rsqrt(mean + EPS) * gain
    other = jnp.where(lane % 2 == 1, pltpu.roll(wide, 1, 1), pltpu.roll(wide, 127, 1))
    return wide * cosine + other * sine


def attention_kernel(
    q_ref, k_ref, v_ref, qg_ref, kg_ref, cos_ref, sin_ref, w_ref, t_ref, whole_ref,
    kv, qz, top, total, acc, own, send_sem, recv_sem, w_sem, t_sem,
):
    me = lax.axis_index("sp")
    core = me % 2
    x = (me // 2) % NX
    z = me // (2 * NX)
    y = lax.axis_index("tp")
    y_up, y_far, y_down = (y + 1) % NY, (y + 2) % NY, (y + 3) % NY

    def slot_of(zz, xx, cc):
        return ((zz % NZ) * NX + xx % NX) * 2 + cc

    partner = slot_of(z, x, 1 - core)
    x_up, x_down = slot_of(z, x + 1, core), slot_of(z, x + NX - 1, core)
    z_up, z_down = slot_of(z + 1, x, core), slot_of(z + NZ - 1, x, core)

    barrier = pltpu.get_barrier_semaphore()
    for there in (partner, x_up, x_down, z_up, z_down):
        pl.semaphore_signal(
            barrier, inc=1, device_id={"sp": there}, device_id_type=pl.DeviceIdType.MESH
        )

    for there in (y_up, y_far, y_down):
        pl.semaphore_signal(
            barrier, inc=1, device_id={"tp": there}, device_id_type=pl.DeviceIdType.MESH
        )

    def share(source, there):
        part = whole_ref.at[pl.ds(pl.multiple_of(source * 256, 256), 256)]
        return pltpu.make_async_remote_copy(
            src_ref=part,
            dst_ref=part,
            send_sem=send_sem.at[1],
            recv_sem=w_sem.at[source],
            device_id={"tp": there},
            device_id_type=pl.DeviceIdType.MESH,
        )

    cosine, sine = cos_ref[...], sin_ref[...]
    turned = normalize_turn(k_ref[...].astype(jnp.float32), kg_ref[...], cosine, sine).astype(
        jnp.bfloat16
    )
    values_t = v_ref[...].astype(jnp.float32).T.astype(jnp.bfloat16)
    for i in range(2):
        kv[me, i, 0:HALF, :] = turned[i * HALF : (i + 1) * HALF]
        kv[me, i, HALF : 2 * HALF, :] = values_t[:, i * HALF : (i + 1) * HALF]
    whole_ref[pl.ds(pl.multiple_of(y * 256, 256), 256), :] = w_ref[...]
    pl.semaphore_wait(barrier, 8)

    def copy(slot, there):
        return pltpu.make_async_remote_copy(
            src_ref=kv.at[slot],
            dst_ref=kv.at[slot],
            send_sem=send_sem.at[0],
            recv_sem=recv_sem.at[slot],
            device_id={"sp": there},
            device_id_type=pl.DeviceIdType.MESH,
        )

    def arrived(slot):
        copy(slot, partner).wait_recv()

    def steps(n):
        near = n - NX
        kz = jnp.where(n < NX, 0, 2 * (near // (2 * NX)) + 1 + near % 2)
        kz = jnp.where(n < CHIPS - NX, kz, NZ - 1)
        kx = jnp.where(n < NX, n, (near % (2 * NX)) // 2)
        kx = jnp.where(n < CHIPS - NX, kx, n % NX)
        zz = z + NZ + (1 - 2 * (kz % 2)) * ((kz + 1) // 2)
        xx = x + NX + (1 - 2 * (kx % 2)) * ((kx + 1) // 2)
        return kz, kx, zz, xx

    def move(n):
        kz, kx, zz, xx = steps(n)
        slot = slot_of(zz, xx, core)

        @pl.when(n > 0)
        def _():
            arrived(slot)

        z_long = jnp.where(core == 0, kx % 2, 0)
        x_long = jnp.where(core == 0, 1, kz % 2)
        z_plus = (kz == 0) | ((kz % 2 == 1) & (kz < 5)) | ((kz == 5) & (z_long == 1))
        z_minus = (kz == 0) | ((kz % 2 == 0) & (kz < 6)) | ((kz == 6) & (z_long == 0))
        x_plus = (kx == 0) | ((kx == 1) & (x_long == 1))
        x_minus = (kx == 0) | ((kx == 2) & (x_long == 0))
        on_z = (core == 0) | (kx == 0)
        on_x = (core == 1) | (kz == 0)

        @pl.when(on_z & z_plus)
        def _():
            copy(slot, z_up).start()

        @pl.when(on_z & z_minus)
        def _():
            copy(slot, z_down).start()

        @pl.when(on_x & x_plus)
        def _():
            copy(slot, x_up).start()

        @pl.when(on_x & x_minus)
        def _():
            copy(slot, x_down).start()

        copy(slot, partner).start()

    move(0)
    share(y, y_up).start()
    share(y, y_down).start()

    for h in range(2):
        part = q_ref[:, h * 128 : (h + 1) * 128].astype(jnp.float32)
        rows = normalize_turn(part, qg_ref[...], cosine, sine).astype(jnp.bfloat16)
        across = (rows.astype(jnp.float32).T * 0.125).astype(jnp.bfloat16)
        qz[h, h * 64 : (h + 1) * 64, 0:256] = across[0:64]
        qz[h, h * 64 : (h + 1) * 64, 256:512] = across[64:128]
        qz[h, (1 - h) * 64 : (2 - h) * 64, :] = jnp.zeros((64, 512), jnp.bfloat16)
    top[...] = jnp.full(top.shape, -1e30, jnp.float32)
    total[...] = jnp.zeros(total.shape, jnp.float32)
    acc[...] = jnp.zeros(acc.shape, jnp.float32)

    for n in range(1, CHUNK + AHEAD):
        move(n)

    def body(step, carry):
        for i in range(CHUNK):
            n = step * CHUNK + CHUNK + AHEAD + i

            @pl.when(n < CHIPS)
            def _():
                move(n)

        @pl.when(step == WEIGHTS_AT // CHUNK)
        def _():
            share(y_down, y_up).wait_recv()
            share(y_up, y_down).wait_recv()

            @pl.when(core == 0)
            def _():
                share(y_down, y_up).start()

            @pl.when(core == 1)
            def _():
                share(y_up, y_down).start()

        blocks = []
        for i in range(CHUNK):
            _, _, zz, xx = steps(step * CHUNK + i)
            arrived(slot_of(zz, xx, 1 - core))
            first = slot_of(zz, xx, 0)
            blocks += [kv.at[first + c, j] for c in range(2) for j in range(2)]
        keys = jnp.concatenate([b[0:HALF, :] for b in blocks], axis=0)
        scores = [jnp.dot(keys, qz[h], preferred_element_type=jnp.float32) for h in range(2)]
        for h in range(2):
            old = top[h]
            new = jnp.maximum(old, jnp.max(scores[h], axis=0, keepdims=True))
            weights = jnp.exp(scores[h] - new)
            shrink = jnp.exp(old - new)
            top[h] = new
            total[h] = total[h] * shrink + jnp.sum(weights, axis=0, keepdims=True)
            vt = jnp.concatenate(
                [b[HALF + h * 64 : HALF + (h + 1) * 64, :] for b in blocks], axis=1
            )
            acc[h] = acc[h] * shrink + jnp.dot(
                vt, weights.astype(jnp.bfloat16), preferred_element_type=jnp.float32
            )
        return carry

    lax.fori_loop(0, CHIPS // CHUNK, body, 0)
    parts = []
    for h in range(2):
        mixed = acc[h] / total[h]
        parts += [mixed[:, 0:256], mixed[:, 256:512]]
    own[...] = jnp.concatenate(parts, axis=0).T.astype(jnp.bfloat16)

    def rows(source, there):
        columns = pl.ds(pl.multiple_of(source * 256, 256), 256)
        return pltpu.make_async_remote_copy(
            src_ref=own.at[pl.ds(pl.multiple_of(there * 64, 64), 64)],
            dst_ref=t_ref.at[:, columns],
            send_sem=send_sem.at[2],
            recv_sem=t_sem.at[source],
            device_id={"tp": there},
            device_id_type=pl.DeviceIdType.MESH,
        )

    for there in (y_far, y_up, y_down):
        rows(y, there).start()
    t_ref[:, pl.ds(pl.multiple_of(y * 256, 256), 256)] = own[
        pl.ds(pl.multiple_of(y * 64, 64), 64), :
    ]
    everything = kv.at[pl.ds(0, 63)]
    pltpu.make_async_copy(everything, everything, send_sem.at[0]).wait()
    share(y_far, y_up).wait_recv()
    three = whole_ref.at[pl.ds(0, 768)]
    pltpu.make_async_copy(three, three, send_sem.at[1]).wait()
    for there in (y_down, y_up, y_far):
        rows(there, y_up).wait_recv()
    three = own.at[pl.ds(0, 192)]
    pltpu.make_async_copy(three, three, send_sem.at[2]).wait()


def attention(queries, keys, values, query_gain, key_gain, cosine, sine, out_rows):
    vmem = pl.BlockSpec(memory_space=pltpu.VMEM)
    return pl.pallas_call(
        attention_kernel,
        out_shape=(
            jax.ShapeDtypeStruct((64, 1024), jnp.bfloat16),
            jax.ShapeDtypeStruct((1024, 2048), jnp.bfloat16),
        ),
        in_specs=[vmem] * 8,
        out_specs=(vmem, vmem),
        scratch_shapes=[
            pltpu.VMEM((2 * CHIPS, 2, 2 * HALF, 128), jnp.bfloat16),
            pltpu.VMEM((2, 128, 512), jnp.bfloat16),
            pltpu.VMEM((2, 1, 512), jnp.float32),
            pltpu.VMEM((2, 1, 512), jnp.float32),
            pltpu.VMEM((2, 64, 512), jnp.float32),
            pltpu.VMEM((256, 256), jnp.bfloat16),
            pltpu.SemaphoreType.DMA((3,)),
            pltpu.SemaphoreType.DMA((2 * CHIPS,)),
            pltpu.SemaphoreType.DMA((NY,)),
            pltpu.SemaphoreType.DMA((NY,)),
        ],
        compiler_params=pltpu.CompilerParams(
            collective_id=0, has_side_effects=True, vmem_limit_bytes=40 * 2**20
        ),
        cost_estimate=pl.CostEstimate(
            flops=8 * 10**9, bytes_accessed=2**20, transcendentals=2**24
        ),
        name="attention",
    )(queries, keys, values, query_gain, key_gain, cosine, sine, out_rows)


def places():
    me = lax.axis_index("sp")
    core, x, z = me % 2, (me // 2) % NX, me // (2 * NX)

    def there(position, sign):
        g, dx, dc = position // 8, (position // 2) % 4, position % 2
        dz = (1 - 2 * (g % 2)) * ((g + 1) // 2)
        zz, xx = (z + sign * dz + NZ) % NZ, (x + sign * dx + NX) % NX
        return (zz * NX + xx) * 2 + (core + dc) % 2

    return me, core, lax.axis_index("tp"), there


def meet_all(there, y):
    barrier = pltpu.get_barrier_semaphore()

    def greet(p, carry):
        pl.semaphore_signal(
            barrier, inc=1, device_id={"sp": there(p, 1)}, device_id_type=pl.DeviceIdType.MESH
        )
        return carry

    lax.fori_loop(1, 64, greet, 0)
    for other in ((y + 1) % NY, (y + 3) % NY):
        pl.semaphore_signal(
            barrier, inc=1, device_id={"tp": other}, device_id_type=pl.DeviceIdType.MESH
        )
    return barrier


def swap_matrix():
    r = lax.broadcasted_iota(jnp.int32, (256, 256), 0)
    c = lax.broadcasted_iota(jnp.int32, (256, 256), 1)
    hit = (r // 16 == c % 16) & (r % 16 == c // 16)
    return jnp.where(hit, 1.0, 0.0).astype(jnp.bfloat16)


def to_tiles(swap, rows):
    stacked = jnp.concatenate([rows[:, j * 128 : (j + 1) * 128] for j in range(16)], axis=0)
    return jnp.dot(swap, stacked, preferred_element_type=jnp.float32).astype(jnp.bfloat16)


def from_tiles(swap, tiles, out_ref, first):
    stacked = jnp.dot(swap, tiles, preferred_element_type=jnp.float32).astype(jnp.bfloat16)
    for j in range(16):
        out_ref[pl.ds(first, 16), j * 128 : (j + 1) * 128] = stacked[j * 16 : (j + 1) * 16]


def block(position):
    return pl.ds(pl.multiple_of(position * 48, 16), 48)


def remote(src, dst, send, recv, **where):
    return pltpu.make_async_remote_copy(
        src_ref=src,
        dst_ref=dst,
        send_sem=send,
        recv_sem=recv,
        device_id=where,
        device_id_type=pl.DeviceIdType.MESH,
    )


def dispatch_kernel(out_ref, x_ref, packed, rows, send_sem, recv_sem, y_sem):
    me, core, y, there = places()
    y_up, y_down = (y + 1) % NY, (y + 3) % NY
    barrier = meet_all(there, y)
    swap = swap_matrix()

    def pack(s, carry):
        first = pl.multiple_of(s * 16, 16)
        packed[pl.ds(pl.multiple_of(s * 256, 256), 256), :] = to_tiles(
            swap, out_ref[pl.ds(first, 16), :]
        )
        return carry

    lax.fori_loop(0, 12, pack, 0)
    rows[0:48, :] = packed[block(me), :]
    pl.semaphore_wait(barrier, 65)

    def hand_out(p, carry):
        to = there(p, 1)
        remote(
            packed.at[block(to)], rows.at[block(p)], send_sem.at[0], recv_sem.at[p], sp=to
        ).start()
        return carry

    lax.fori_loop(1, 64, hand_out, 0)

    def await_row(p, carry):
        remote(
            packed.at[block(p)], rows.at[block(p)], send_sem.at[0], recv_sem.at[p], sp=me
        ).wait_recv()
        return carry

    def part(relative, k):
        return rows.at[pl.ds(pl.multiple_of(relative * 3072 + k * 768, 256), 768)]

    def along(relative_from, relative_to, k, to):
        return remote(
            part(relative_from, k), part(relative_to, k),
            send_sem.at[1], y_sem.at[relative_to, k], tp=to,
        )

    def pass_on(k):
        along(0, 1, k, y_up).wait_recv()
        along(0, 3, k, y_down).wait_recv()

        @pl.when(core == 0)
        def _():
            along(1, 2, k, y_up).start()

        @pl.when(core == 1)
        def _():
            along(3, 2, k, y_down).start()

    def spread(k, carry):
        lax.fori_loop(jnp.maximum(16 * k, 1), 16 * k + 16, await_row, 0)
        along(0, 1, k, y_up).start()
        along(0, 3, k, y_down).start()

        @pl.when(k > 0)
        def _():
            pass_on(k - 1)

        return carry

    lax.fori_loop(0, 4, spread, 0)
    pass_on(3)

    def unpack(s, carry):
        tiles = rows[pl.ds(pl.multiple_of(s * 256, 256), 256), :]
        from_tiles(swap, tiles, x_ref, pl.multiple_of(s * 16, 16))
        return carry

    lax.fori_loop(0, 24, unpack, 0)
    lax.fori_loop(36, 48, unpack, 0)
    for k in range(4):
        along(0, 2, k, y_up).wait_recv()
    lax.fori_loop(24, 36, unpack, 0)
    sent = packed.at[pl.ds(0, 63 * 48)]
    pltpu.make_async_copy(sent, sent, send_sem.at[0]).wait()
    sent = rows.at[pl.ds(0, 9216)]
    pltpu.make_async_copy(sent, sent, send_sem.at[1]).wait()


def dispatch(outgoing):
    vmem = pl.BlockSpec(memory_space=pltpu.VMEM)
    return pl.pallas_call(
        dispatch_kernel,
        out_shape=jax.ShapeDtypeStruct((768, 2048), jnp.bfloat16),
        in_specs=[vmem],
        out_specs=vmem,
        scratch_shapes=[
            pltpu.VMEM((3072, 128), jnp.bfloat16),
            pltpu.VMEM((12288, 128), jnp.bfloat16),
            pltpu.SemaphoreType.DMA((2,)),
            pltpu.SemaphoreType.DMA((64,)),
            pltpu.SemaphoreType.DMA((NY, 4)),
        ],
        compiler_params=pltpu.CompilerParams(
            collective_id=1, has_side_effects=True, vmem_limit_bytes=24 * 2**20
        ),
        name="dispatch",
    )(outgoing)


def combine_kernel(
    p_ref, back_ref, far, near, both, summed, packed, returned, send_sem, recv_sem, y_sem
):
    me, core, y, there = places()
    ahead, behind = (y + 1 + 2 * core) % NY, (y + 3 - 2 * core) % NY
    to_ahead, to_behind = 3 - 2 * core, 1 + 2 * core
    barrier = meet_all(there, y)
    swap = swap_matrix()
    pl.semaphore_wait(barrier, 65)

    def chunk(k):
        return pl.ds(pl.multiple_of(k * 48, 16), 48)

    def partial(relative, k):
        return pl.ds(pl.multiple_of(relative * 192 + k * 48, 16), 48)

    def send_far(k):
        return remote(
            p_ref.at[partial(2, k)], far.at[chunk(k)], send_sem.at[0], y_sem.at[0, k], tp=ahead
        )

    def send_near(k):
        return remote(
            p_ref.at[partial(to_behind, k)], near.at[chunk(k)],
            send_sem.at[0], y_sem.at[1, k], tp=behind,
        )

    def send_both(k):
        return remote(
            summed.at[chunk(k)], both.at[chunk(k)], send_sem.at[0], y_sem.at[2, k], tp=ahead
        )

    def send_back(p):
        return remote(
            packed.at[block(p)], returned.at[block(me)], send_sem.at[1], recv_sem.at[p],
            sp=there(p, -1),
        )

    for k in range(4):
        send_far(k).start()
        send_near(k).start()

    def finish(k):
        send_near(k).wait_recv()
        send_both(k).wait_recv()

        def pack(s, carry):
            first = pl.ds(pl.multiple_of(k * 48 + s * 16, 16), 16)
            answer = (
                p_ref[first, :].astype(jnp.float32)
                + near[first, :].astype(jnp.float32)
                + both[first, :].astype(jnp.float32)
            ).astype(jnp.bfloat16)
            packed[pl.ds(pl.multiple_of(k * 768 + s * 256, 256), 256), :] = to_tiles(swap, answer)
            return carry

        lax.fori_loop(0, 3, pack, 0)

        def give_back(p, carry):
            send_back(p).start()
            return carry

        lax.fori_loop(jnp.maximum(16 * k, 1), 16 * k + 16, give_back, 0)

    def reduce(k, carry):
        send_far(k).wait_recv()
        summed[chunk(k), :] = (
            p_ref[partial(to_ahead, k), :].astype(jnp.float32)
            + far[chunk(k), :].astype(jnp.float32)
        ).astype(jnp.bfloat16)
        send_both(k).start()

        @pl.when(k > 0)
        def _():
            finish(k - 1)

        return carry

    lax.fori_loop(0, 4, reduce, 0)
    finish(3)
    returned[block(me), :] = packed[0:48, :]

    def await_row(p, carry):
        source = there(p, 1)
        remote(
            packed.at[block(p)], returned.at[block(source)], send_sem.at[1], recv_sem.at[p], sp=source
        ).wait_recv()
        return carry

    lax.fori_loop(1, 64, await_row, 0)

    def unpack(s, carry):
        tiles = returned[pl.ds(pl.multiple_of(s * 256, 256), 256), :]
        from_tiles(swap, tiles, back_ref, pl.multiple_of(s * 16, 16))
        return carry

    lax.fori_loop(0, 12, unpack, 0)
    sent = p_ref.at[pl.ds(0, 576)]
    pltpu.make_async_copy(sent, sent, send_sem.at[0]).wait()
    sent = packed.at[pl.ds(0, 63 * 48)]
    pltpu.make_async_copy(sent, sent, send_sem.at[1]).wait()


def combine(partials):
    vmem = pl.BlockSpec(memory_space=pltpu.VMEM)
    third = pltpu.VMEM((192, 2048), jnp.bfloat16)
    return pl.pallas_call(
        combine_kernel,
        out_shape=jax.ShapeDtypeStruct((192, 2048), jnp.bfloat16),
        in_specs=[vmem],
        out_specs=vmem,
        scratch_shapes=[
            third, third, third, third,
            pltpu.VMEM((3072, 128), jnp.bfloat16),
            pltpu.VMEM((3072, 128), jnp.bfloat16),
            pltpu.SemaphoreType.DMA((2,)),
            pltpu.SemaphoreType.DMA((64,)),
            pltpu.SemaphoreType.DMA((3, 4)),
        ],
        compiler_params=pltpu.CompilerParams(
            collective_id=2, has_side_effects=True, vmem_limit_bytes=24 * 2**20
        ),
        name="combine",
    )(partials)


def local(
    stream_in, queries, keys, values, query_gain, key_gain, out_rows, norm_gain,
    route_ids, route_weights, gate_weight, up_weight, down_weight,
):
    head_size = query_gain.shape[0]
    seq_rows = queries.shape[0]
    cosine, sine = turn_tables(lax.axis_index("sp") * seq_rows, seq_rows, head_size)
    twice = lambda g: jnp.tile(g, 2)[None, :]
    token_heads, whole_out = attention(
        queries, keys, values, twice(query_gain), twice(key_gain), cosine, sine, out_rows
    )
    projected = jnp.dot(token_heads, whole_out, preferred_element_type=jnp.float32)
    stream = (stream_in.astype(jnp.float32) + projected).astype(jnp.bfloat16)
    stream_wide = stream.astype(jnp.float32)
    normed = (
        stream_wide
        * lax.rsqrt(jnp.mean(stream_wide * stream_wide, axis=1, keepdims=True) + EPS)
        * norm_gain
    ).astype(jnp.bfloat16)
    tokens = stream.shape[0]
    model_width = stream.shape[1]
    top_count = route_ids.shape[1]
    experts = lax.axis_size("sp")
    routed = tokens * top_count
    capacity = SLOTS
    flat_ids = route_ids.reshape(routed)
    member = (flat_ids[:, None] == jnp.arange(experts, dtype=jnp.int32)[None, :]).astype(jnp.int32)
    earlier = jnp.cumsum(member, axis=0) - member
    slot_rank = jnp.sum(earlier * member, axis=1)
    target = flat_ids * capacity + slot_rank
    placed = (target[:, None] == jnp.arange(experts * capacity, dtype=jnp.int32)[None, :]).astype(
        jnp.bfloat16
    )
    placed = placed.reshape(tokens, top_count, experts * capacity)
    outgoing = jnp.einsum("tks,td->sd", placed, normed, preferred_element_type=jnp.float32).astype(
        jnp.bfloat16
    )
    row_piece = dispatch(outgoing)
    gate_value = jnp.dot(row_piece, gate_weight[0], preferred_element_type=jnp.float32)
    up_value = jnp.dot(row_piece, up_weight[0], preferred_element_type=jnp.float32)
    hidden = (jax.nn.silu(gate_value) * up_value).astype(jnp.bfloat16)
    partials = jnp.dot(hidden, down_weight[0], preferred_element_type=jnp.float32)
    expert_back = combine(partials.astype(jnp.bfloat16))
    picked = jnp.einsum("tks,sd->tkd", placed, expert_back, preferred_element_type=jnp.float32)
    mixed_out = stream_wide + jnp.sum(route_weights[:, :, None] * picked, axis=1)
    return mixed_out.astype(jnp.bfloat16)


def solution(mesh):
    return jax.shard_map(
        local,
        mesh=mesh,
        in_specs=(
            P(("sp", "tp"), None),
            P("sp", "tp"),
            P("sp", "tp"),
            P("sp", "tp"),
            P(),
            P(),
            P("tp", None),
            P(),
            P(("sp", "tp"), None),
            P(("sp", "tp"), None),
            P("sp", None, "tp"),
            P("sp", None, "tp"),
            P("sp", "tp", None),
        ),
        out_specs=P(("sp", "tp"), None),
        check_vma=False,
    )
```

```python
import jax
import jax.numpy as jnp
from jax import lax
from jax.experimental import pallas as pl
from jax.experimental.pallas import tpu as pltpu
from jax.sharding import PartitionSpec as P

GRID_W = 64
EPS = 1e-06
THETA = 10000.0
NZ, NX, NY = 8, 4, 4
CHIPS = NZ * NX
CHUNK = 1
AHEAD = 3
WEIGHTS_AT = 16
SLOTS = 3
HALF = 128


def turn_tables(offset, count, head_size):
    position = offset + jnp.arange(count, dtype=jnp.int32)
    grid_row = (position // GRID_W).astype(jnp.float32)
    column = (position % GRID_W).astype(jnp.float32)
    pair_index = jnp.arange(head_size // 4, dtype=jnp.float32)
    inverse = THETA ** (-4.0 * pair_index / head_size)
    lane = jnp.arange(2 * head_size, dtype=jnp.int32) % head_size
    pair = lane // 2
    wide_inverse = jnp.tile(jnp.repeat(inverse, 2), 4)
    place = jnp.where((pair < head_size // 4)[None, :], grid_row[:, None], column[:, None])
    angles = place * wide_inverse
    sign = jnp.where(lane % 2 == 1, 1.0, -1.0)
    return jnp.cos(angles), jnp.sin(angles) * sign


def normalize_turn(x, gain, cosine, sine):
    lane = lax.broadcasted_iota(jnp.int32, x.shape, 1)
    low = lane < 64
    squares = x * x
    first = jnp.sum(jnp.where(low, squares, 0.0), axis=1, keepdims=True)
    second = jnp.sum(jnp.where(low, 0.0, squares), axis=1, keepdims=True)
    mean = jnp.where(low, first, second) * (1.0 / 64)
    wide = x * lax.rsqrt(mean + EPS) * gain
    other = jnp.where(lane % 2 == 1, pltpu.roll(wide, 1, 1), pltpu.roll(wide, 127, 1))
    return wide * cosine + other * sine


def attention_kernel(
    q_ref, k_ref, v_ref, qg_ref, kg_ref, cos_ref, sin_ref, w_ref, t_ref, whole_ref,
    kv, qz, top, total, acc, own, send_sem, recv_sem, w_sem, t_sem,
):
    me = lax.axis_index("sp")
    core = me % 2
    x = (me // 2) % NX
    z = me // (2 * NX)
    y = lax.axis_index("tp")
    y_up, y_far, y_down = (y + 1) % NY, (y + 2) % NY, (y + 3) % NY

    def slot_of(zz, xx, cc):
        return ((zz % NZ) * NX + xx % NX) * 2 + cc

    partner = slot_of(z, x, 1 - core)
    x_up, x_down = slot_of(z, x + 1, core), slot_of(z, x + NX - 1, core)
    z_up, z_down = slot_of(z + 1, x, core), slot_of(z + NZ - 1, x, core)

    barrier = pltpu.get_barrier_semaphore()
    for there in (partner, x_up, x_down, z_up, z_down):
        pl.semaphore_signal(
            barrier, inc=1, device_id={"sp": there}, device_id_type=pl.DeviceIdType.MESH
        )

    for there in (y_up, y_far, y_down):
        pl.semaphore_signal(
            barrier, inc=1, device_id={"tp": there}, device_id_type=pl.DeviceIdType.MESH
        )

    def share(source, there):
        part = whole_ref.at[pl.ds(pl.multiple_of(source * 256, 256), 256)]
        return pltpu.make_async_remote_copy(
            src_ref=part,
            dst_ref=part,
            send_sem=send_sem.at[1],
            recv_sem=w_sem.at[source],
            device_id={"tp": there},
            device_id_type=pl.DeviceIdType.MESH,
        )

    cosine, sine = cos_ref[...], sin_ref[...]
    turned = normalize_turn(k_ref[...].astype(jnp.float32), kg_ref[...], cosine, sine).astype(
        jnp.bfloat16
    )
    values_t = v_ref[...].astype(jnp.float32).T.astype(jnp.bfloat16)
    for i in range(2):
        kv[me, i, 0:HALF, :] = turned[i * HALF : (i + 1) * HALF]
        kv[me, i, HALF : 2 * HALF, :] = values_t[:, i * HALF : (i + 1) * HALF]
    whole_ref[pl.ds(pl.multiple_of(y * 256, 256), 256), :] = w_ref[...]
    pl.semaphore_wait(barrier, 8)

    def copy(slot, there):
        return pltpu.make_async_remote_copy(
            src_ref=kv.at[slot],
            dst_ref=kv.at[slot],
            send_sem=send_sem.at[0],
            recv_sem=recv_sem.at[slot],
            device_id={"sp": there},
            device_id_type=pl.DeviceIdType.MESH,
        )

    def arrived(slot):
        copy(slot, partner).wait_recv()

    def steps(n):
        near = n - NX
        kz = jnp.where(n < NX, 0, 2 * (near // (2 * NX)) + 1 + near % 2)
        kz = jnp.where(n < CHIPS - NX, kz, NZ - 1)
        kx = jnp.where(n < NX, n, (near % (2 * NX)) // 2)
        kx = jnp.where(n < CHIPS - NX, kx, n % NX)
        zz = z + NZ + (1 - 2 * (kz % 2)) * ((kz + 1) // 2)
        xx = x + NX + (1 - 2 * (kx % 2)) * ((kx + 1) // 2)
        return kz, kx, zz, xx

    def move(n):
        kz, kx, zz, xx = steps(n)
        slot = slot_of(zz, xx, core)

        @pl.when(n > 0)
        def _():
            arrived(slot)

        z_long = jnp.where(core == 0, kx % 2, 0)
        x_long = jnp.where(core == 0, 1, kz % 2)
        z_plus = (kz == 0) | ((kz % 2 == 1) & (kz < 5)) | ((kz == 5) & (z_long == 1))
        z_minus = (kz == 0) | ((kz % 2 == 0) & (kz < 6)) | ((kz == 6) & (z_long == 0))
        x_plus = (kx == 0) | ((kx == 1) & (x_long == 1))
        x_minus = (kx == 0) | ((kx == 2) & (x_long == 0))
        on_z = (core == 0) | (kx == 0)
        on_x = (core == 1) | (kz == 0)

        @pl.when(on_z & z_plus)
        def _():
            copy(slot, z_up).start()

        @pl.when(on_z & z_minus)
        def _():
            copy(slot, z_down).start()

        @pl.when(on_x & x_plus)
        def _():
            copy(slot, x_up).start()

        @pl.when(on_x & x_minus)
        def _():
            copy(slot, x_down).start()

        copy(slot, partner).start()

    move(0)
    share(y, y_up).start()
    share(y, y_down).start()

    for h in range(2):
        part = q_ref[:, h * 128 : (h + 1) * 128].astype(jnp.float32)
        rows = normalize_turn(part, qg_ref[...], cosine, sine).astype(jnp.bfloat16)
        across = (rows.astype(jnp.float32).T * 0.125).astype(jnp.bfloat16)
        qz[h, h * 64 : (h + 1) * 64, 0:256] = across[0:64]
        qz[h, h * 64 : (h + 1) * 64, 256:512] = across[64:128]
        qz[h, (1 - h) * 64 : (2 - h) * 64, :] = jnp.zeros((64, 512), jnp.bfloat16)
    top[...] = jnp.full(top.shape, -1e30, jnp.float32)
    total[...] = jnp.zeros(total.shape, jnp.float32)
    acc[...] = jnp.zeros(acc.shape, jnp.float32)

    for n in range(1, CHUNK + AHEAD):
        move(n)

    def body(step, carry):
        for i in range(CHUNK):
            n = step * CHUNK + CHUNK + AHEAD + i

            @pl.when(n < CHIPS)
            def _():
                move(n)

        @pl.when(step == WEIGHTS_AT // CHUNK)
        def _():
            share(y_down, y_up).wait_recv()
            share(y_up, y_down).wait_recv()

            @pl.when(core == 0)
            def _():
                share(y_down, y_up).start()

            @pl.when(core == 1)
            def _():
                share(y_up, y_down).start()

        blocks = []
        for i in range(CHUNK):
            _, _, zz, xx = steps(step * CHUNK + i)
            arrived(slot_of(zz, xx, 1 - core))
            first = slot_of(zz, xx, 0)
            blocks += [kv.at[first + c, j] for c in range(2) for j in range(2)]
        keys = jnp.concatenate([b[0:HALF, :] for b in blocks], axis=0)
        scores = [jnp.dot(keys, qz[h], preferred_element_type=jnp.float32) for h in range(2)]
        for h in range(2):
            old = top[h]
            new = jnp.maximum(old, jnp.max(scores[h], axis=0, keepdims=True))
            weights = jnp.exp(scores[h] - new)
            shrink = jnp.exp(old - new)
            top[h] = new
            total[h] = total[h] * shrink + jnp.sum(weights, axis=0, keepdims=True)
            vt = jnp.concatenate(
                [b[HALF + h * 64 : HALF + (h + 1) * 64, :] for b in blocks], axis=1
            )
            acc[h] = acc[h] * shrink + jnp.dot(
                vt, weights.astype(jnp.bfloat16), preferred_element_type=jnp.float32
            )
        return carry

    lax.fori_loop(0, CHIPS // CHUNK, body, 0)
    parts = []
    for h in range(2):
        mixed = acc[h] / total[h]
        parts += [mixed[:, 0:256], mixed[:, 256:512]]
    own[...] = jnp.concatenate(parts, axis=0).T.astype(jnp.bfloat16)

    def rows(source, there):
        columns = pl.ds(pl.multiple_of(source * 256, 256), 256)
        return pltpu.make_async_remote_copy(
            src_ref=own.at[pl.ds(pl.multiple_of(there * 64, 64), 64)],
            dst_ref=t_ref.at[:, columns],
            send_sem=send_sem.at[2],
            recv_sem=t_sem.at[source],
            device_id={"tp": there},
            device_id_type=pl.DeviceIdType.MESH,
        )

    for there in (y_far, y_up, y_down):
        rows(y, there).start()
    t_ref[:, pl.ds(pl.multiple_of(y * 256, 256), 256)] = own[
        pl.ds(pl.multiple_of(y * 64, 64), 64), :
    ]
    everything = kv.at[pl.ds(0, 63)]
    pltpu.make_async_copy(everything, everything, send_sem.at[0]).wait()
    share(y_far, y_up).wait_recv()
    three = whole_ref.at[pl.ds(0, 768)]
    pltpu.make_async_copy(three, three, send_sem.at[1]).wait()
    for there in (y_down, y_up, y_far):
        rows(there, y_up).wait_recv()
    three = own.at[pl.ds(0, 192)]
    pltpu.make_async_copy(three, three, send_sem.at[2]).wait()


def attention(queries, keys, values, query_gain, key_gain, cosine, sine, out_rows):
    vmem = pl.BlockSpec(memory_space=pltpu.VMEM)
    return pl.pallas_call(
        attention_kernel,
        out_shape=(
            jax.ShapeDtypeStruct((64, 1024), jnp.bfloat16),
            jax.ShapeDtypeStruct((1024, 2048), jnp.bfloat16),
        ),
        in_specs=[vmem] * 8,
        out_specs=(vmem, vmem),
        scratch_shapes=[
            pltpu.VMEM((2 * CHIPS, 2, 2 * HALF, 128), jnp.bfloat16),
            pltpu.VMEM((2, 128, 512), jnp.bfloat16),
            pltpu.VMEM((2, 1, 512), jnp.float32),
            pltpu.VMEM((2, 1, 512), jnp.float32),
            pltpu.VMEM((2, 64, 512), jnp.float32),
            pltpu.VMEM((256, 256), jnp.bfloat16),
            pltpu.SemaphoreType.DMA((3,)),
            pltpu.SemaphoreType.DMA((2 * CHIPS,)),
            pltpu.SemaphoreType.DMA((NY,)),
            pltpu.SemaphoreType.DMA((NY,)),
        ],
        compiler_params=pltpu.CompilerParams(
            collective_id=0, has_side_effects=True, vmem_limit_bytes=40 * 2**20
        ),
        cost_estimate=pl.CostEstimate(
            flops=8 * 10**9, bytes_accessed=2**20, transcendentals=2**24
        ),
        name="attention",
    )(queries, keys, values, query_gain, key_gain, cosine, sine, out_rows)


def places():
    me = lax.axis_index("sp")
    core, x, z = me % 2, (me // 2) % NX, me // (2 * NX)

    def there(position, sign):
        g, dx, dc = position // 8, (position // 2) % 4, position % 2
        dz = (1 - 2 * (g % 2)) * ((g + 1) // 2)
        zz, xx = (z + sign * dz + NZ) % NZ, (x + sign * dx + NX) % NX
        return (zz * NX + xx) * 2 + (core + dc) % 2

    return me, core, lax.axis_index("tp"), there


def meet_all(there, y):
    barrier = pltpu.get_barrier_semaphore()

    def greet(p, carry):
        pl.semaphore_signal(
            barrier, inc=1, device_id={"sp": there(p, 1)}, device_id_type=pl.DeviceIdType.MESH
        )
        return carry

    lax.fori_loop(1, 64, greet, 0)
    for other in ((y + 1) % NY, (y + 3) % NY):
        pl.semaphore_signal(
            barrier, inc=1, device_id={"tp": other}, device_id_type=pl.DeviceIdType.MESH
        )
    return barrier


def swap_matrix():
    r = lax.broadcasted_iota(jnp.int32, (256, 256), 0)
    c = lax.broadcasted_iota(jnp.int32, (256, 256), 1)
    hit = (r // 16 == c % 16) & (r % 16 == c // 16)
    return jnp.where(hit, 1.0, 0.0).astype(jnp.bfloat16)


def to_tiles(swap, rows):
    stacked = jnp.concatenate([rows[:, j * 128 : (j + 1) * 128] for j in range(16)], axis=0)
    return jnp.dot(swap, stacked, preferred_element_type=jnp.float32).astype(jnp.bfloat16)


def from_tiles(swap, tiles, out_ref, first):
    stacked = jnp.dot(swap, tiles, preferred_element_type=jnp.float32).astype(jnp.bfloat16)
    for j in range(16):
        out_ref[pl.ds(first, 16), j * 128 : (j + 1) * 128] = stacked[j * 16 : (j + 1) * 16]


def block(position):
    return pl.ds(pl.multiple_of(position * 48, 16), 48)


def remote(src, dst, send, recv, **where):
    return pltpu.make_async_remote_copy(
        src_ref=src,
        dst_ref=dst,
        send_sem=send,
        recv_sem=recv,
        device_id=where,
        device_id_type=pl.DeviceIdType.MESH,
    )


def experts_kernel(
    out_ref, gate_hbm, up_hbm, down_hbm, back_ref,
    gate, up, down, packed, rows, x_rows, hidden, parts, far, near, both, summed, answers, returned,
    load_sem, send_sem, out_sem, spread_sem, sum_sem, back_sem,
):
    me, core, y, there = places()
    y_up, y_down = (y + 1) % NY, (y + 3) % NY
    ahead, behind = (y + 1 + 2 * core) % NY, (y + 3 - 2 * core) % NY
    to_ahead, to_behind = 3 - 2 * core, 1 + 2 * core
    barrier = meet_all(there, y)
    loads = [
        pltpu.make_async_copy(src, dst, load_sem.at[i])
        for i, (src, dst) in enumerate(((gate_hbm, gate), (up_hbm, up), (down_hbm, down)))
    ]
    for load in loads:
        load.start()
    swap = swap_matrix()

    def tiles_at(first):
        return pl.ds(pl.multiple_of(first, 256), 256)

    def pack(s, carry):
        first = pl.multiple_of(s * 16, 16)
        packed[tiles_at(s * 256), :] = to_tiles(swap, out_ref[pl.ds(first, 16), :])
        return carry

    lax.fori_loop(0, 12, pack, 0)
    rows[0:48, :] = packed[block(me), :]
    pl.semaphore_wait(barrier, 65)

    def hand_out(p, carry):
        to = there(p, 1)
        remote(
            packed.at[block(to)], rows.at[block(p)], send_sem.at[0], out_sem.at[p], sp=to
        ).start()
        return carry

    lax.fori_loop(1, 64, hand_out, 0)

    def part(relative, k):
        return rows.at[pl.ds(pl.multiple_of(relative * 3072 + k * 768, 256), 768)]

    def along(relative_from, relative_to, k, to):
        return remote(
            part(relative_from, k), part(relative_to, k),
            send_sem.at[1], spread_sem.at[relative_to, k], tp=to,
        )

    def await_row(p, carry):
        remote(
            packed.at[block(p)], rows.at[block(p)], send_sem.at[0], out_sem.at[p], sp=me
        ).wait_recv()
        return carry

    def spread(k):
        lax.fori_loop(jnp.maximum(16 * k, 1), 16 * k + 16, await_row, 0)
        along(0, 1, k, y_up).start()
        along(0, 3, k, y_down).start()

    def pass_on(k):
        along(0, 1, k, y_up).wait_recv()
        along(0, 3, k, y_down).wait_recv()

        @pl.when(core == 0)
        def _():
            along(1, 2, k, y_up).start()

        @pl.when(core == 1)
        def _():
            along(3, 2, k, y_down).start()

    def chunk(k):
        return pl.ds(pl.multiple_of(k * 48, 16), 48)

    def partial(relative, k):
        return pl.ds(pl.multiple_of(k * 192 + relative * 48, 16), 48)

    def send_far(k):
        return remote(
            parts.at[partial(2, k)], far.at[chunk(k)], send_sem.at[2], sum_sem.at[0, k], tp=ahead
        )

    def send_near(k):
        return remote(
            parts.at[partial(to_behind, k)], near.at[chunk(k)],
            send_sem.at[2], sum_sem.at[1, k], tp=behind,
        )

    def send_both(k):
        return remote(
            summed.at[chunk(k)], both.at[chunk(k)], send_sem.at[2], sum_sem.at[2, k], tp=ahead
        )

    def compute(k):
        along(0, 2, k, y_up).wait_recv()

        def unpack_x(i, carry):
            relative, s = i // 3, i % 3
            tiles = rows[tiles_at(relative * 3072 + k * 768 + s * 256), :]
            from_tiles(swap, tiles, x_rows, pl.multiple_of(i * 16, 16))
            return carry

        lax.fori_loop(0, 12, unpack_x, 0)
        mine = x_rows[...]
        for n in range(3):
            columns = slice(n * 256, (n + 1) * 256)
            gated = jnp.dot(mine, gate[:, columns], preferred_element_type=jnp.float32)
            upped = jnp.dot(mine, up[:, columns], preferred_element_type=jnp.float32)
            hidden[:, columns] = (gated / (1.0 + jnp.exp(-gated)) * upped).astype(jnp.bfloat16)
        units = hidden[...]
        for n in range(8):
            columns = slice(n * 256, (n + 1) * 256)
            parts[pl.ds(pl.multiple_of(k * 192, 16), 192), columns] = jnp.dot(
                units, down[:, columns], preferred_element_type=jnp.float32
            ).astype(jnp.bfloat16)
        send_far(k).start()
        send_near(k).start()

    def add_far(k):
        send_far(k).wait_recv()
        summed[chunk(k), :] = (
            parts[partial(to_ahead, k), :].astype(jnp.float32)
            + far[chunk(k), :].astype(jnp.float32)
        ).astype(jnp.bfloat16)
        send_both(k).start()

    def finish(k):
        send_near(k).wait_recv()
        send_both(k).wait_recv()

        def pack_answer(s, carry):
            own = pl.ds(pl.multiple_of(k * 192 + s * 16, 16), 16)
            arrived = pl.ds(pl.multiple_of(k * 48 + s * 16, 16), 16)
            answer = (
                parts[own, :].astype(jnp.float32)
                + near[arrived, :].astype(jnp.float32)
                + both[arrived, :].astype(jnp.float32)
            ).astype(jnp.bfloat16)
            answers[tiles_at(k * 768 + s * 256), :] = to_tiles(swap, answer)
            return carry

        lax.fori_loop(0, 3, pack_answer, 0)

        def give_back(p, carry):
            remote(
                answers.at[block(p)], returned.at[block(me)], send_sem.at[3], back_sem.at[p],
                sp=there(p, -1),
            ).start()
            return carry

        lax.fori_loop(jnp.maximum(16 * k, 1), 16 * k + 16, give_back, 0)

    def tick(t, carry):
        @pl.when(t < 4)
        def _():
            spread(t)

        @pl.when((t >= 1) & (t < 5))
        def _():
            pass_on(t - 1)

        @pl.when(t == 2)
        def _():
            for load in loads:
                load.wait()

        @pl.when((t >= 3) & (t < 7))
        def _():
            add_far(t - 3)

        @pl.when((t >= 2) & (t < 6))
        def _():
            compute(t - 2)

        @pl.when(t >= 4)
        def _():
            finish(t - 4)

        return carry

    lax.fori_loop(0, 8, tick, 0)
    returned[block(me), :] = answers[0:48, :]

    def await_back(p, carry):
        source = there(p, 1)
        remote(
            answers.at[block(p)], returned.at[block(source)], send_sem.at[3], back_sem.at[p],
            sp=source,
        ).wait_recv()
        return carry

    lax.fori_loop(1, 64, await_back, 0)

    def unpack(s, carry):
        from_tiles(swap, returned[tiles_at(s * 256), :], back_ref, pl.multiple_of(s * 16, 16))
        return carry

    lax.fori_loop(0, 12, unpack, 0)
    for i, sent in enumerate((
        packed.at[pl.ds(0, 63 * 48)],
        rows.at[pl.ds(0, 9216)],
        parts.at[pl.ds(0, 576)],
        answers.at[pl.ds(0, 63 * 48)],
    )):
        pltpu.make_async_copy(sent, sent, send_sem.at[i]).wait()


def expert_layer(outgoing, gate, up, down):
    vmem = pl.BlockSpec(memory_space=pltpu.VMEM)
    hbm = pl.BlockSpec(memory_space=pltpu.HBM)

    def room(*shape):
        return pltpu.VMEM(shape, jnp.bfloat16)

    return pl.pallas_call(
        experts_kernel,
        out_shape=jax.ShapeDtypeStruct((192, 2048), jnp.bfloat16),
        in_specs=[vmem, hbm, hbm, hbm],
        out_specs=vmem,
        scratch_shapes=[
            room(2048, 768), room(2048, 768), room(768, 2048),
            room(3072, 128), room(12288, 128), room(192, 2048), room(192, 768), room(768, 2048),
            room(192, 2048), room(192, 2048), room(192, 2048), room(192, 2048),
            room(3072, 128), room(3072, 128),
            pltpu.SemaphoreType.DMA((3,)),
            pltpu.SemaphoreType.DMA((4,)),
            pltpu.SemaphoreType.DMA((64,)),
            pltpu.SemaphoreType.DMA((NY, 4)),
            pltpu.SemaphoreType.DMA((3, 4)),
            pltpu.SemaphoreType.DMA((64,)),
        ],
        compiler_params=pltpu.CompilerParams(
            collective_id=1, has_side_effects=True, vmem_limit_bytes=56 * 2**20
        ),
        name="experts",
    )(outgoing, gate, up, down)


def local(
    stream_in, queries, keys, values, query_gain, key_gain, out_rows, norm_gain,
    route_ids, route_weights, gate_weight, up_weight, down_weight,
):
    head_size = query_gain.shape[0]
    seq_rows = queries.shape[0]
    cosine, sine = turn_tables(lax.axis_index("sp") * seq_rows, seq_rows, head_size)
    twice = lambda g: jnp.tile(g, 2)[None, :]
    token_heads, whole_out = attention(
        queries, keys, values, twice(query_gain), twice(key_gain), cosine, sine, out_rows
    )
    projected = jnp.dot(token_heads, whole_out, preferred_element_type=jnp.float32)
    stream = (stream_in.astype(jnp.float32) + projected).astype(jnp.bfloat16)
    stream_wide = stream.astype(jnp.float32)
    normed = (
        stream_wide
        * lax.rsqrt(jnp.mean(stream_wide * stream_wide, axis=1, keepdims=True) + EPS)
        * norm_gain
    ).astype(jnp.bfloat16)
    tokens = stream.shape[0]
    model_width = stream.shape[1]
    top_count = route_ids.shape[1]
    experts = lax.axis_size("sp")
    routed = tokens * top_count
    capacity = SLOTS
    flat_ids = route_ids.reshape(routed)
    member = (flat_ids[:, None] == jnp.arange(experts, dtype=jnp.int32)[None, :]).astype(jnp.int32)
    earlier = jnp.cumsum(member, axis=0) - member
    slot_rank = jnp.sum(earlier * member, axis=1)
    target = flat_ids * capacity + slot_rank
    placed = (target[:, None] == jnp.arange(experts * capacity, dtype=jnp.int32)[None, :]).astype(
        jnp.bfloat16
    )
    placed = placed.reshape(tokens, top_count, experts * capacity)
    outgoing = jnp.einsum("tks,td->sd", placed, normed, preferred_element_type=jnp.float32).astype(
        jnp.bfloat16
    )
    expert_back = expert_layer(outgoing, gate_weight[0], up_weight[0], down_weight[0])
    picked = jnp.einsum("tks,sd->tkd", placed, expert_back, preferred_element_type=jnp.float32)
    mixed_out = stream_wide + jnp.sum(route_weights[:, :, None] * picked, axis=1)
    return mixed_out.astype(jnp.bfloat16)


def solution(mesh):
    return jax.shard_map(
        local,
        mesh=mesh,
        in_specs=(
            P(("sp", "tp"), None),
            P("sp", "tp"),
            P("sp", "tp"),
            P("sp", "tp"),
            P(),
            P(),
            P("tp", None),
            P(),
            P(("sp", "tp"), None),
            P(("sp", "tp"), None),
            P("sp", None, "tp"),
            P("sp", None, "tp"),
            P("sp", "tp", None),
        ),
        out_specs=P(("sp", "tp"), None),
        check_vma=False,
    )
```

```python
import jax
import jax.numpy as jnp
from jax import lax
from jax.experimental import pallas as pl
from jax.experimental.pallas import tpu as pltpu
from jax.sharding import PartitionSpec as P

GRID_W = 64
EPS = 1e-06
THETA = 10000.0
NZ, NX, NY = 8, 4, 4
CHIPS = NZ * NX
CHUNK = 1
AHEAD = 3
WEIGHTS_AT = 20
SLOTS = 3
HALF = 128


def turn_tables(offset, count, head_size):
    position = offset + jnp.arange(count, dtype=jnp.int32)
    grid_row = (position // GRID_W).astype(jnp.float32)
    column = (position % GRID_W).astype(jnp.float32)
    pair_index = jnp.arange(head_size // 4, dtype=jnp.float32)
    inverse = THETA ** (-4.0 * pair_index / head_size)
    lane = jnp.arange(2 * head_size, dtype=jnp.int32) % head_size
    pair = lane // 2
    wide_inverse = jnp.tile(jnp.repeat(inverse, 2), 4)
    place = jnp.where((pair < head_size // 4)[None, :], grid_row[:, None], column[:, None])
    angles = place * wide_inverse
    sign = jnp.where(lane % 2 == 1, 1.0, -1.0)
    return jnp.cos(angles), jnp.sin(angles) * sign


def normalize_turn(x, gain, cosine, sine):
    lane = lax.broadcasted_iota(jnp.int32, x.shape, 1)
    low = lane < 64
    squares = x * x
    first = jnp.sum(jnp.where(low, squares, 0.0), axis=1, keepdims=True)
    second = jnp.sum(jnp.where(low, 0.0, squares), axis=1, keepdims=True)
    mean = jnp.where(low, first, second) * (1.0 / 64)
    wide = x * lax.rsqrt(mean + EPS) * gain
    other = jnp.where(lane % 2 == 1, pltpu.roll(wide, 1, 1), pltpu.roll(wide, 127, 1))
    return wide * cosine + other * sine


def attention_kernel(
    q_ref, k_ref, v_ref, qg_ref, kg_ref, cos_ref, sin_ref, w_ref, t_ref, whole_ref,
    kv, qz, top, total, acc, own, send_sem, recv_sem, w_sem, t_sem,
):
    me = lax.axis_index("sp")
    core = me % 2
    x = (me // 2) % NX
    z = me // (2 * NX)
    y = lax.axis_index("tp")
    y_up, y_far, y_down = (y + 1) % NY, (y + 2) % NY, (y + 3) % NY

    def slot_of(zz, xx, cc):
        return ((zz % NZ) * NX + xx % NX) * 2 + cc

    partner = slot_of(z, x, 1 - core)
    x_up, x_down = slot_of(z, x + 1, core), slot_of(z, x + NX - 1, core)
    z_up, z_down = slot_of(z + 1, x, core), slot_of(z + NZ - 1, x, core)

    barrier = pltpu.get_barrier_semaphore()
    for there in (partner, x_up, x_down, z_up, z_down):
        pl.semaphore_signal(
            barrier, inc=1, device_id={"sp": there}, device_id_type=pl.DeviceIdType.MESH
        )

    for there in (y_up, y_far, y_down):
        pl.semaphore_signal(
            barrier, inc=1, device_id={"tp": there}, device_id_type=pl.DeviceIdType.MESH
        )

    def share(source, there):
        part = whole_ref.at[pl.ds(pl.multiple_of(source * 256, 256), 256)]
        return pltpu.make_async_remote_copy(
            src_ref=part,
            dst_ref=part,
            send_sem=send_sem.at[1],
            recv_sem=w_sem.at[source],
            device_id={"tp": there},
            device_id_type=pl.DeviceIdType.MESH,
        )

    cosine, sine = cos_ref[...], sin_ref[...]
    turned = normalize_turn(k_ref[...].astype(jnp.float32), kg_ref[...], cosine, sine).astype(
        jnp.bfloat16
    )
    values_t = v_ref[...].astype(jnp.float32).T.astype(jnp.bfloat16)
    for i in range(2):
        kv[me, i, 0:HALF, :] = turned[i * HALF : (i + 1) * HALF]
        kv[me, i, HALF : 2 * HALF, :] = values_t[:, i * HALF : (i + 1) * HALF]
    whole_ref[pl.ds(pl.multiple_of(y * 256, 256), 256), :] = w_ref[...]
    pl.semaphore_wait(barrier, 8)

    def copy(slot, there):
        return pltpu.make_async_remote_copy(
            src_ref=kv.at[slot],
            dst_ref=kv.at[slot],
            send_sem=send_sem.at[0],
            recv_sem=recv_sem.at[slot],
            device_id={"sp": there},
            device_id_type=pl.DeviceIdType.MESH,
        )

    def arrived(slot):
        copy(slot, partner).wait_recv()

    def steps(n):
        near = n - NX
        kz = jnp.where(n < NX, 0, 2 * (near // (2 * NX)) + 1 + near % 2)
        kz = jnp.where(n < CHIPS - NX, kz, NZ - 1)
        kx = jnp.where(n < NX, n, (near % (2 * NX)) // 2)
        kx = jnp.where(n < CHIPS - NX, kx, n % NX)
        zz = z + NZ + (1 - 2 * (kz % 2)) * ((kz + 1) // 2)
        xx = x + NX + (1 - 2 * (kx % 2)) * ((kx + 1) // 2)
        return kz, kx, zz, xx

    def move(n):
        kz, kx, zz, xx = steps(n)
        slot = slot_of(zz, xx, core)

        @pl.when(n > 0)
        def _():
            arrived(slot)

        z_long = jnp.where(core == 0, kx % 2, 0)
        x_long = jnp.where(core == 0, 1, kz % 2)
        z_plus = (kz == 0) | ((kz % 2 == 1) & (kz < 5)) | ((kz == 5) & (z_long == 1))
        z_minus = (kz == 0) | ((kz % 2 == 0) & (kz < 6)) | ((kz == 6) & (z_long == 0))
        x_plus = (kx == 0) | ((kx == 1) & (x_long == 1))
        x_minus = (kx == 0) | ((kx == 2) & (x_long == 0))
        on_z = (core == 0) | (kx == 0)
        on_x = (core == 1) | (kz == 0)

        @pl.when(on_z & z_plus)
        def _():
            copy(slot, z_up).start()

        @pl.when(on_z & z_minus)
        def _():
            copy(slot, z_down).start()

        @pl.when(on_x & x_plus)
        def _():
            copy(slot, x_up).start()

        @pl.when(on_x & x_minus)
        def _():
            copy(slot, x_down).start()

        copy(slot, partner).start()

    move(0)
    share(y, y_up).start()
    share(y, y_down).start()

    for h in range(2):
        part = q_ref[:, h * 128 : (h + 1) * 128].astype(jnp.float32)
        rows = normalize_turn(part, qg_ref[...], cosine, sine).astype(jnp.bfloat16)
        across = (rows.astype(jnp.float32).T * 0.125).astype(jnp.bfloat16)
        qz[h, h * 64 : (h + 1) * 64, 0:256] = across[0:64]
        qz[h, h * 64 : (h + 1) * 64, 256:512] = across[64:128]
        qz[h, (1 - h) * 64 : (2 - h) * 64, :] = jnp.zeros((64, 512), jnp.bfloat16)
    top[...] = jnp.full(top.shape, -1e30, jnp.float32)
    total[...] = jnp.zeros(total.shape, jnp.float32)
    acc[...] = jnp.zeros(acc.shape, jnp.float32)

    for n in range(1, CHUNK + AHEAD):
        move(n)

    def body(step, carry):
        for i in range(CHUNK):
            n = step * CHUNK + CHUNK + AHEAD + i

            @pl.when(n < CHIPS)
            def _():
                move(n)

        @pl.when(step == WEIGHTS_AT // CHUNK)
        def _():
            share(y_down, y_up).wait_recv()
            share(y_up, y_down).wait_recv()

            @pl.when(core == 0)
            def _():
                share(y_down, y_up).start()

            @pl.when(core == 1)
            def _():
                share(y_up, y_down).start()

        blocks = []
        for i in range(CHUNK):
            _, _, zz, xx = steps(step * CHUNK + i)
            arrived(slot_of(zz, xx, 1 - core))
            first = slot_of(zz, xx, 0)
            blocks += [kv.at[first + c, j] for c in range(2) for j in range(2)]
        keys = jnp.concatenate([b[0:HALF, :] for b in blocks], axis=0)
        scores = [jnp.dot(keys, qz[h], preferred_element_type=jnp.float32) for h in range(2)]
        for h in range(2):
            old = top[h]
            new = jnp.maximum(old, jnp.max(scores[h], axis=0, keepdims=True))
            weights = jnp.exp(scores[h] - new)
            shrink = jnp.exp(old - new)
            top[h] = new
            total[h] = total[h] * shrink + jnp.sum(weights, axis=0, keepdims=True)
            vt = jnp.concatenate(
                [b[HALF + h * 64 : HALF + (h + 1) * 64, :] for b in blocks], axis=1
            )
            acc[h] = acc[h] * shrink + jnp.dot(
                vt, weights.astype(jnp.bfloat16), preferred_element_type=jnp.float32
            )
        return carry

    lax.fori_loop(0, CHIPS // CHUNK, body, 0)
    parts = []
    for h in range(2):
        mixed = acc[h] / total[h]
        parts += [mixed[:, 0:256], mixed[:, 256:512]]
    own[...] = jnp.concatenate(parts, axis=0).T.astype(jnp.bfloat16)

    def rows(source, there):
        columns = pl.ds(pl.multiple_of(source * 256, 256), 256)
        return pltpu.make_async_remote_copy(
            src_ref=own.at[pl.ds(pl.multiple_of(there * 64, 64), 64)],
            dst_ref=t_ref.at[:, columns],
            send_sem=send_sem.at[2],
            recv_sem=t_sem.at[source],
            device_id={"tp": there},
            device_id_type=pl.DeviceIdType.MESH,
        )

    for there in (y_far, y_up, y_down):
        rows(y, there).start()
    t_ref[:, pl.ds(pl.multiple_of(y * 256, 256), 256)] = own[
        pl.ds(pl.multiple_of(y * 64, 64), 64), :
    ]
    everything = kv.at[pl.ds(0, 63)]
    pltpu.make_async_copy(everything, everything, send_sem.at[0]).wait()
    share(y_far, y_up).wait_recv()
    three = whole_ref.at[pl.ds(0, 768)]
    pltpu.make_async_copy(three, three, send_sem.at[1]).wait()
    for there in (y_down, y_up, y_far):
        rows(there, y_up).wait_recv()
    three = own.at[pl.ds(0, 192)]
    pltpu.make_async_copy(three, three, send_sem.at[2]).wait()


def attention(queries, keys, values, query_gain, key_gain, cosine, sine, out_rows):
    vmem = pl.BlockSpec(memory_space=pltpu.VMEM)
    return pl.pallas_call(
        attention_kernel,
        out_shape=(
            jax.ShapeDtypeStruct((64, 1024), jnp.bfloat16),
            jax.ShapeDtypeStruct((1024, 2048), jnp.bfloat16),
        ),
        in_specs=[vmem] * 8,
        out_specs=(vmem, vmem),
        scratch_shapes=[
            pltpu.VMEM((2 * CHIPS, 2, 2 * HALF, 128), jnp.bfloat16),
            pltpu.VMEM((2, 128, 512), jnp.bfloat16),
            pltpu.VMEM((2, 1, 512), jnp.float32),
            pltpu.VMEM((2, 1, 512), jnp.float32),
            pltpu.VMEM((2, 64, 512), jnp.float32),
            pltpu.VMEM((256, 256), jnp.bfloat16),
            pltpu.SemaphoreType.DMA((3,)),
            pltpu.SemaphoreType.DMA((2 * CHIPS,)),
            pltpu.SemaphoreType.DMA((NY,)),
            pltpu.SemaphoreType.DMA((NY,)),
        ],
        compiler_params=pltpu.CompilerParams(
            collective_id=0, has_side_effects=True, vmem_limit_bytes=40 * 2**20
        ),
        cost_estimate=pl.CostEstimate(
            flops=8 * 10**9, bytes_accessed=2**20, transcendentals=2**24
        ),
        name="attention",
    )(queries, keys, values, query_gain, key_gain, cosine, sine, out_rows)


def places():
    me = lax.axis_index("sp")
    core, x, z = me % 2, (me // 2) % NX, me // (2 * NX)

    def there(position, sign):
        g, dx, dc = position // 8, (position // 2) % 4, position % 2
        dz = (1 - 2 * (g % 2)) * ((g + 1) // 2)
        zz, xx = (z + sign * dz + NZ) % NZ, (x + sign * dx + NX) % NX
        return (zz * NX + xx) * 2 + (core + dc) % 2

    return me, core, lax.axis_index("tp"), there


def meet_all(there, y):
    barrier = pltpu.get_barrier_semaphore()

    def greet(p, carry):
        pl.semaphore_signal(
            barrier, inc=1, device_id={"sp": there(p, 1)}, device_id_type=pl.DeviceIdType.MESH
        )
        return carry

    lax.fori_loop(1, 64, greet, 0)
    for other in ((y + 1) % NY, (y + 3) % NY):
        pl.semaphore_signal(
            barrier, inc=1, device_id={"tp": other}, device_id_type=pl.DeviceIdType.MESH
        )
    return barrier


def swap_matrix():
    r = lax.broadcasted_iota(jnp.int32, (256, 256), 0)
    c = lax.broadcasted_iota(jnp.int32, (256, 256), 1)
    hit = (r // 16 == c % 16) & (r % 16 == c // 16)
    return jnp.where(hit, 1.0, 0.0).astype(jnp.bfloat16)


def to_tiles(swap, rows):
    stacked = jnp.concatenate([rows[:, j * 128 : (j + 1) * 128] for j in range(16)], axis=0)
    return jnp.dot(swap, stacked, preferred_element_type=jnp.float32).astype(jnp.bfloat16)


def from_tiles(swap, tiles, out_ref, first):
    stacked = jnp.dot(swap, tiles, preferred_element_type=jnp.float32).astype(jnp.bfloat16)
    for j in range(16):
        out_ref[pl.ds(first, 16), j * 128 : (j + 1) * 128] = stacked[j * 16 : (j + 1) * 16]


def block(position):
    return pl.ds(pl.multiple_of(position * 48, 16), 48)


def remote(src, dst, send, recv, **where):
    return pltpu.make_async_remote_copy(
        src_ref=src,
        dst_ref=dst,
        send_sem=send,
        recv_sem=recv,
        device_id=where,
        device_id_type=pl.DeviceIdType.MESH,
    )


def experts_kernel(
    out_ref, gate_hbm, up_hbm, down_hbm, back_ref,
    gate, up, down, packed, rows, x_rows, hidden, parts, far, near, both, summed, answers, returned,
    load_sem, send_sem, out_sem, spread_sem, sum_sem, back_sem,
):
    me, core, y, there = places()
    y_up, y_down = (y + 1) % NY, (y + 3) % NY
    ahead, behind = (y + 1 + 2 * core) % NY, (y + 3 - 2 * core) % NY
    to_ahead, to_behind = 3 - 2 * core, 1 + 2 * core
    barrier = meet_all(there, y)
    loads = [
        pltpu.make_async_copy(src, dst, load_sem.at[i])
        for i, (src, dst) in enumerate(((gate_hbm, gate), (up_hbm, up), (down_hbm, down)))
    ]
    for load in loads:
        load.start()
    swap = swap_matrix()

    def tiles_at(first):
        return pl.ds(pl.multiple_of(first, 256), 256)

    def pack(s, carry):
        first = pl.multiple_of(s * 16, 16)
        packed[tiles_at(s * 256), :] = to_tiles(swap, out_ref[pl.ds(first, 16), :])
        return carry

    lax.fori_loop(0, 12, pack, 0)
    rows[0:48, :] = packed[block(me), :]
    pl.semaphore_wait(barrier, 65)

    def hand_out(i, carry):
        p = (i + 16) % 64
        to = there(p, 1)

        @pl.when(p > 0)
        def _():
            remote(
                packed.at[block(to)], rows.at[block(p)], send_sem.at[0], out_sem.at[p], sp=to
            ).start()

        return carry

    lax.fori_loop(0, 64, hand_out, 0)

    def part(relative, k):
        return rows.at[pl.ds(pl.multiple_of(relative * 3072 + k * 768, 256), 768)]

    def along(relative_from, relative_to, k, to):
        return remote(
            part(relative_from, k), part(relative_to, k),
            send_sem.at[1], spread_sem.at[relative_to, k], tp=to,
        )

    def await_row(p, carry):
        remote(
            packed.at[block(p)], rows.at[block(p)], send_sem.at[0], out_sem.at[p], sp=me
        ).wait_recv()
        return carry

    def spread(k):
        lax.fori_loop(jnp.maximum(16 * k, 1), 16 * k + 16, await_row, 0)
        along(0, 1, k, y_up).start()
        along(0, 3, k, y_down).start()

    def pass_on(k):
        along(0, 1, k, y_up).wait_recv()
        along(0, 3, k, y_down).wait_recv()

        @pl.when(core == 0)
        def _():
            along(1, 2, k, y_up).start()

        @pl.when(core == 1)
        def _():
            along(3, 2, k, y_down).start()

    def chunk(k):
        return pl.ds(pl.multiple_of(k * 48, 16), 48)

    def partial(relative, k):
        return pl.ds(pl.multiple_of(k * 192 + relative * 48, 16), 48)

    def send_far(k):
        return remote(
            parts.at[partial(2, k)], far.at[chunk(k)], send_sem.at[2], sum_sem.at[0, k], tp=ahead
        )

    def send_near(k):
        return remote(
            parts.at[partial(to_behind, k)], near.at[chunk(k)],
            send_sem.at[2], sum_sem.at[1, k], tp=behind,
        )

    def send_both(k):
        return remote(
            summed.at[chunk(k)], both.at[chunk(k)], send_sem.at[2], sum_sem.at[2, k], tp=ahead
        )

    def compute(k):
        along(0, 2, k, y_up).wait_recv()

        def unpack_x(i, carry):
            relative, s = i // 3, i % 3
            tiles = rows[tiles_at(relative * 3072 + k * 768 + s * 256), :]
            from_tiles(swap, tiles, x_rows, pl.multiple_of(i * 16, 16))
            return carry

        lax.fori_loop(0, 12, unpack_x, 0)
        mine = x_rows[...]
        for n in range(3):
            columns = slice(n * 256, (n + 1) * 256)
            gated = jnp.dot(mine, gate[:, columns], preferred_element_type=jnp.float32)
            upped = jnp.dot(mine, up[:, columns], preferred_element_type=jnp.float32)
            hidden[:, columns] = (gated / (1.0 + jnp.exp(-gated)) * upped).astype(jnp.bfloat16)
        units = hidden[...]
        for n in range(8):
            columns = slice(n * 256, (n + 1) * 256)
            parts[pl.ds(pl.multiple_of(k * 192, 16), 192), columns] = jnp.dot(
                units, down[:, columns], preferred_element_type=jnp.float32
            ).astype(jnp.bfloat16)
        send_far(k).start()
        send_near(k).start()

    def add_far(k):
        send_far(k).wait_recv()
        summed[chunk(k), :] = (
            parts[partial(to_ahead, k), :].astype(jnp.float32)
            + far[chunk(k), :].astype(jnp.float32)
        ).astype(jnp.bfloat16)
        send_both(k).start()

    def finish(k):
        send_near(k).wait_recv()
        send_both(k).wait_recv()

        def pack_answer(s, carry):
            own = pl.ds(pl.multiple_of(k * 192 + s * 16, 16), 16)
            arrived = pl.ds(pl.multiple_of(k * 48 + s * 16, 16), 16)
            answer = (
                parts[own, :].astype(jnp.float32)
                + near[arrived, :].astype(jnp.float32)
                + both[arrived, :].astype(jnp.float32)
            ).astype(jnp.bfloat16)
            answers[tiles_at(k * 768 + s * 256), :] = to_tiles(swap, answer)
            return carry

        lax.fori_loop(0, 3, pack_answer, 0)

        def give_back(p, carry):
            remote(
                answers.at[block(p)], returned.at[block(me)], send_sem.at[3], back_sem.at[p],
                sp=there(p, -1),
            ).start()
            return carry

        lax.fori_loop(jnp.maximum(16 * k, 1), 16 * k + 16, give_back, 0)

    def tick(t, carry):
        @pl.when(t < 4)
        def _():
            spread((t + 1) % 4)

        @pl.when((t >= 1) & (t < 5))
        def _():
            pass_on(t % 4)

        @pl.when(t == 2)
        def _():
            for load in loads:
                load.wait()

        @pl.when((t >= 2) & (t < 6))
        def _():
            compute((t - 1) % 4)

        @pl.when((t >= 3) & (t < 7))
        def _():
            add_far((t - 2) % 4)

        @pl.when(t >= 4)
        def _():
            finish((t - 3) % 4)

        return carry

    lax.fori_loop(0, 8, tick, 0)
    returned[block(me), :] = answers[0:48, :]

    def await_back(p, carry):
        source = there(p, 1)
        remote(
            answers.at[block(p)], returned.at[block(source)], send_sem.at[3], back_sem.at[p],
            sp=source,
        ).wait_recv()
        return carry

    lax.fori_loop(1, 64, await_back, 0)

    def unpack(s, carry):
        from_tiles(swap, returned[tiles_at(s * 256), :], back_ref, pl.multiple_of(s * 16, 16))
        return carry

    lax.fori_loop(0, 12, unpack, 0)
    for i, sent in enumerate((
        packed.at[pl.ds(0, 63 * 48)],
        rows.at[pl.ds(0, 9216)],
        parts.at[pl.ds(0, 576)],
        answers.at[pl.ds(0, 63 * 48)],
    )):
        pltpu.make_async_copy(sent, sent, send_sem.at[i]).wait()


def expert_layer(outgoing, gate, up, down):
    vmem = pl.BlockSpec(memory_space=pltpu.VMEM)
    hbm = pl.BlockSpec(memory_space=pltpu.HBM)

    def room(*shape):
        return pltpu.VMEM(shape, jnp.bfloat16)

    return pl.pallas_call(
        experts_kernel,
        out_shape=jax.ShapeDtypeStruct((192, 2048), jnp.bfloat16),
        in_specs=[vmem, hbm, hbm, hbm],
        out_specs=vmem,
        scratch_shapes=[
            room(2048, 768), room(2048, 768), room(768, 2048),
            room(3072, 128), room(12288, 128), room(192, 2048), room(192, 768), room(768, 2048),
            room(192, 2048), room(192, 2048), room(192, 2048), room(192, 2048),
            room(3072, 128), room(3072, 128),
            pltpu.SemaphoreType.DMA((3,)),
            pltpu.SemaphoreType.DMA((4,)),
            pltpu.SemaphoreType.DMA((64,)),
            pltpu.SemaphoreType.DMA((NY, 4)),
            pltpu.SemaphoreType.DMA((3, 4)),
            pltpu.SemaphoreType.DMA((64,)),
        ],
        compiler_params=pltpu.CompilerParams(
            collective_id=1, has_side_effects=True, vmem_limit_bytes=56 * 2**20
        ),
        name="experts",
    )(outgoing, gate, up, down)


def local(
    stream_in, queries, keys, values, query_gain, key_gain, out_rows, norm_gain,
    route_ids, route_weights, gate_weight, up_weight, down_weight,
):
    head_size = query_gain.shape[0]
    seq_rows = queries.shape[0]
    cosine, sine = turn_tables(lax.axis_index("sp") * seq_rows, seq_rows, head_size)
    twice = lambda g: jnp.tile(g, 2)[None, :]
    token_heads, whole_out = attention(
        queries, keys, values, twice(query_gain), twice(key_gain), cosine, sine, out_rows
    )
    projected = jnp.dot(token_heads, whole_out, preferred_element_type=jnp.float32)
    stream = (stream_in.astype(jnp.float32) + projected).astype(jnp.bfloat16)
    stream_wide = stream.astype(jnp.float32)
    normed = (
        stream_wide
        * lax.rsqrt(jnp.mean(stream_wide * stream_wide, axis=1, keepdims=True) + EPS)
        * norm_gain
    ).astype(jnp.bfloat16)
    tokens = stream.shape[0]
    model_width = stream.shape[1]
    top_count = route_ids.shape[1]
    experts = lax.axis_size("sp")
    routed = tokens * top_count
    capacity = SLOTS
    flat_ids = route_ids.reshape(routed)
    member = (flat_ids[:, None] == jnp.arange(experts, dtype=jnp.int32)[None, :]).astype(jnp.int32)
    earlier = jnp.cumsum(member, axis=0) - member
    slot_rank = jnp.sum(earlier * member, axis=1)
    target = flat_ids * capacity + slot_rank
    placed = (target[:, None] == jnp.arange(experts * capacity, dtype=jnp.int32)[None, :]).astype(
        jnp.bfloat16
    )
    placed = placed.reshape(tokens, top_count, experts * capacity)
    outgoing = jnp.einsum("tks,td->sd", placed, normed, preferred_element_type=jnp.float32).astype(
        jnp.bfloat16
    )
    expert_back = expert_layer(outgoing, gate_weight[0], up_weight[0], down_weight[0])
    picked = jnp.einsum("tks,sd->tkd", placed, expert_back, preferred_element_type=jnp.float32)
    mixed_out = stream_wide + jnp.sum(route_weights[:, :, None] * picked, axis=1)
    return mixed_out.astype(jnp.bfloat16)


def solution(mesh):
    return jax.shard_map(
        local,
        mesh=mesh,
        in_specs=(
            P(("sp", "tp"), None),
            P("sp", "tp"),
            P("sp", "tp"),
            P("sp", "tp"),
            P(),
            P(),
            P("tp", None),
            P(),
            P(("sp", "tp"), None),
            P(("sp", "tp"), None),
            P("sp", None, "tp"),
            P("sp", None, "tp"),
            P("sp", "tp", None),
        ),
        out_specs=P(("sp", "tp"), None),
        check_vma=False,
    )
```

```python
import jax
import jax.numpy as jnp
from jax import lax
from jax.experimental import pallas as pl
from jax.experimental.pallas import tpu as pltpu
from jax.sharding import PartitionSpec as P

GRID_W = 64
EPS = 1e-06
THETA = 10000.0
NZ, NX, NY = 8, 4, 4
CHIPS = NZ * NX
CHUNK = 1
AHEAD = 4
WEIGHTS_AT = 20
SLOTS = 3
HALF = 128


def turn_tables(offset, count, head_size):
    position = offset + jnp.arange(count, dtype=jnp.int32)
    grid_row = (position // GRID_W).astype(jnp.float32)
    column = (position % GRID_W).astype(jnp.float32)
    pair_index = jnp.arange(head_size // 4, dtype=jnp.float32)
    inverse = THETA ** (-4.0 * pair_index / head_size)
    lane = jnp.arange(2 * head_size, dtype=jnp.int32) % head_size
    pair = lane // 2
    wide_inverse = jnp.tile(jnp.repeat(inverse, 2), 4)
    place = jnp.where((pair < head_size // 4)[None, :], grid_row[:, None], column[:, None])
    angles = place * wide_inverse
    sign = jnp.where(lane % 2 == 1, 1.0, -1.0)
    return jnp.cos(angles), jnp.sin(angles) * sign


def normalize_turn(x, gain, cosine, sine):
    lane = lax.broadcasted_iota(jnp.int32, x.shape, 1)
    low = lane < 64
    squares = x * x
    first = jnp.sum(jnp.where(low, squares, 0.0), axis=1, keepdims=True)
    second = jnp.sum(jnp.where(low, 0.0, squares), axis=1, keepdims=True)
    mean = jnp.where(low, first, second) * (1.0 / 64)
    wide = x * lax.rsqrt(mean + EPS) * gain
    other = jnp.where(lane % 2 == 1, pltpu.roll(wide, 1, 1), pltpu.roll(wide, 127, 1))
    return wide * cosine + other * sine


def attention_kernel(
    q_ref, k_ref, v_ref, qg_ref, kg_ref, cos_ref, sin_ref, w_ref, t_ref, whole_ref,
    kv, qz, top, total, acc, own, send_sem, recv_sem, w_sem, t_sem,
):
    me = lax.axis_index("sp")
    core = me % 2
    x = (me // 2) % NX
    z = me // (2 * NX)
    y = lax.axis_index("tp")
    y_up, y_far, y_down = (y + 1) % NY, (y + 2) % NY, (y + 3) % NY

    def slot_of(zz, xx, cc):
        return ((zz % NZ) * NX + xx % NX) * 2 + cc

    partner = slot_of(z, x, 1 - core)
    x_up, x_down = slot_of(z, x + 1, core), slot_of(z, x + NX - 1, core)
    z_up, z_down = slot_of(z + 1, x, core), slot_of(z + NZ - 1, x, core)

    barrier = pltpu.get_barrier_semaphore()
    for there in (partner, x_up, x_down, z_up, z_down):
        pl.semaphore_signal(
            barrier, inc=1, device_id={"sp": there}, device_id_type=pl.DeviceIdType.MESH
        )

    for there in (y_up, y_far, y_down):
        pl.semaphore_signal(
            barrier, inc=1, device_id={"tp": there}, device_id_type=pl.DeviceIdType.MESH
        )

    def share(source, there):
        part = whole_ref.at[pl.ds(pl.multiple_of(source * 256, 256), 256)]
        return pltpu.make_async_remote_copy(
            src_ref=part,
            dst_ref=part,
            send_sem=send_sem.at[1],
            recv_sem=w_sem.at[source],
            device_id={"tp": there},
            device_id_type=pl.DeviceIdType.MESH,
        )

    cosine, sine = cos_ref[...], sin_ref[...]
    turned = normalize_turn(k_ref[...].astype(jnp.float32), kg_ref[...], cosine, sine).astype(
        jnp.bfloat16
    )
    values_t = v_ref[...].astype(jnp.float32).T.astype(jnp.bfloat16)
    for i in range(2):
        kv[me, i, 0:HALF, :] = turned[i * HALF : (i + 1) * HALF]
        kv[me, i, HALF : 2 * HALF, :] = values_t[:, i * HALF : (i + 1) * HALF]
    whole_ref[pl.ds(pl.multiple_of(y * 256, 256), 256), :] = w_ref[...]
    pl.semaphore_wait(barrier, 8)

    def copy(slot, there):
        return pltpu.make_async_remote_copy(
            src_ref=kv.at[slot],
            dst_ref=kv.at[slot],
            send_sem=send_sem.at[0],
            recv_sem=recv_sem.at[slot],
            device_id={"sp": there},
            device_id_type=pl.DeviceIdType.MESH,
        )

    def arrived(slot):
        copy(slot, partner).wait_recv()

    def steps(n):
        near = n - NX
        kz = jnp.where(n < NX, 0, 2 * (near // (2 * NX)) + 1 + near % 2)
        kz = jnp.where(n < CHIPS - NX, kz, NZ - 1)
        kx = jnp.where(n < NX, n, (near % (2 * NX)) // 2)
        kx = jnp.where(n < CHIPS - NX, kx, n % NX)
        zz = z + NZ + (1 - 2 * (kz % 2)) * ((kz + 1) // 2)
        xx = x + NX + (1 - 2 * (kx % 2)) * ((kx + 1) // 2)
        return kz, kx, zz, xx

    def move(n):
        kz, kx, zz, xx = steps(n)
        slot = slot_of(zz, xx, core)

        @pl.when(n > 0)
        def _():
            arrived(slot)

        z_long = jnp.where(core == 0, kx % 2, 0)
        x_long = jnp.where(core == 0, 1, kz % 2)
        z_plus = (kz == 0) | ((kz % 2 == 1) & (kz < 5)) | ((kz == 5) & (z_long == 1))
        z_minus = (kz == 0) | ((kz % 2 == 0) & (kz < 6)) | ((kz == 6) & (z_long == 0))
        x_plus = (kx == 0) | ((kx == 1) & (x_long == 1))
        x_minus = (kx == 0) | ((kx == 2) & (x_long == 0))
        on_z = (core == 0) | (kx == 0)
        on_x = (core == 1) | (kz == 0)

        @pl.when(on_z & z_plus)
        def _():
            copy(slot, z_up).start()

        @pl.when(on_z & z_minus)
        def _():
            copy(slot, z_down).start()

        @pl.when(on_x & x_plus)
        def _():
            copy(slot, x_up).start()

        @pl.when(on_x & x_minus)
        def _():
            copy(slot, x_down).start()

        copy(slot, partner).start()

    move(0)
    share(y, y_up).start()
    share(y, y_down).start()

    for h in range(2):
        part = q_ref[:, h * 128 : (h + 1) * 128].astype(jnp.float32)
        rows = normalize_turn(part, qg_ref[...], cosine, sine).astype(jnp.bfloat16)
        across = (rows.astype(jnp.float32).T * 0.125).astype(jnp.bfloat16)
        qz[h, h * 64 : (h + 1) * 64, 0:256] = across[0:64]
        qz[h, h * 64 : (h + 1) * 64, 256:512] = across[64:128]
        qz[h, (1 - h) * 64 : (2 - h) * 64, :] = jnp.zeros((64, 512), jnp.bfloat16)
    top[...] = jnp.full(top.shape, -1e30, jnp.float32)
    total[...] = jnp.zeros(total.shape, jnp.float32)
    acc[...] = jnp.zeros(acc.shape, jnp.float32)

    for n in range(1, CHUNK + AHEAD):
        move(n)

    def body(step, carry):
        for i in range(CHUNK):
            n = step * CHUNK + CHUNK + AHEAD + i

            @pl.when(n < CHIPS)
            def _():
                move(n)

        @pl.when(step == WEIGHTS_AT // CHUNK)
        def _():
            share(y_down, y_up).wait_recv()
            share(y_up, y_down).wait_recv()

            @pl.when(core == 0)
            def _():
                share(y_down, y_up).start()

            @pl.when(core == 1)
            def _():
                share(y_up, y_down).start()

        blocks = []
        for i in range(CHUNK):
            _, _, zz, xx = steps(step * CHUNK + i)
            arrived(slot_of(zz, xx, 1 - core))
            first = slot_of(zz, xx, 0)
            blocks += [kv.at[first + c, j] for c in range(2) for j in range(2)]
        keys = jnp.concatenate([b[0:HALF, :] for b in blocks], axis=0)
        scores = [jnp.dot(keys, qz[h], preferred_element_type=jnp.float32) for h in range(2)]
        for h in range(2):
            old = top[h]
            new = jnp.maximum(old, jnp.max(scores[h], axis=0, keepdims=True))
            weights = jnp.exp(scores[h] - new)
            shrink = jnp.exp(old - new)
            top[h] = new
            total[h] = total[h] * shrink + jnp.sum(weights, axis=0, keepdims=True)
            vt = jnp.concatenate(
                [b[HALF + h * 64 : HALF + (h + 1) * 64, :] for b in blocks], axis=1
            )
            acc[h] = acc[h] * shrink + jnp.dot(
                vt, weights.astype(jnp.bfloat16), preferred_element_type=jnp.float32
            )
        return carry

    lax.fori_loop(0, CHIPS // CHUNK, body, 0)
    parts = []
    for h in range(2):
        mixed = acc[h] / total[h]
        parts += [mixed[:, 0:256], mixed[:, 256:512]]
    own[...] = jnp.concatenate(parts, axis=0).T.astype(jnp.bfloat16)

    def rows(source, there):
        columns = pl.ds(pl.multiple_of(source * 256, 256), 256)
        return pltpu.make_async_remote_copy(
            src_ref=own.at[pl.ds(pl.multiple_of(there * 64, 64), 64)],
            dst_ref=t_ref.at[:, columns],
            send_sem=send_sem.at[2],
            recv_sem=t_sem.at[source],
            device_id={"tp": there},
            device_id_type=pl.DeviceIdType.MESH,
        )

    for there in (y_far, y_up, y_down):
        rows(y, there).start()
    t_ref[:, pl.ds(pl.multiple_of(y * 256, 256), 256)] = own[
        pl.ds(pl.multiple_of(y * 64, 64), 64), :
    ]
    everything = kv.at[pl.ds(0, 63)]
    pltpu.make_async_copy(everything, everything, send_sem.at[0]).wait()
    share(y_far, y_up).wait_recv()
    three = whole_ref.at[pl.ds(0, 768)]
    pltpu.make_async_copy(three, three, send_sem.at[1]).wait()
    for there in (y_down, y_up, y_far):
        rows(there, y_up).wait_recv()
    three = own.at[pl.ds(0, 192)]
    pltpu.make_async_copy(three, three, send_sem.at[2]).wait()


def attention(queries, keys, values, query_gain, key_gain, cosine, sine, out_rows):
    vmem = pl.BlockSpec(memory_space=pltpu.VMEM)
    return pl.pallas_call(
        attention_kernel,
        out_shape=(
            jax.ShapeDtypeStruct((64, 1024), jnp.bfloat16),
            jax.ShapeDtypeStruct((1024, 2048), jnp.bfloat16),
        ),
        in_specs=[vmem] * 8,
        out_specs=(vmem, vmem),
        scratch_shapes=[
            pltpu.VMEM((2 * CHIPS, 2, 2 * HALF, 128), jnp.bfloat16),
            pltpu.VMEM((2, 128, 512), jnp.bfloat16),
            pltpu.VMEM((2, 1, 512), jnp.float32),
            pltpu.VMEM((2, 1, 512), jnp.float32),
            pltpu.VMEM((2, 64, 512), jnp.float32),
            pltpu.VMEM((256, 256), jnp.bfloat16),
            pltpu.SemaphoreType.DMA((3,)),
            pltpu.SemaphoreType.DMA((2 * CHIPS,)),
            pltpu.SemaphoreType.DMA((NY,)),
            pltpu.SemaphoreType.DMA((NY,)),
        ],
        compiler_params=pltpu.CompilerParams(
            collective_id=0, has_side_effects=True, vmem_limit_bytes=40 * 2**20
        ),
        cost_estimate=pl.CostEstimate(
            flops=8 * 10**9, bytes_accessed=2**20, transcendentals=2**24
        ),
        name="attention",
    )(queries, keys, values, query_gain, key_gain, cosine, sine, out_rows)


def places():
    me = lax.axis_index("sp")
    core, x, z = me % 2, (me // 2) % NX, me // (2 * NX)

    def there(position, sign):
        g, dx, dc = position // 8, (position // 2) % 4, position % 2
        dz = (1 - 2 * (g % 2)) * ((g + 1) // 2)
        zz, xx = (z + sign * dz + NZ) % NZ, (x + sign * dx + NX) % NX
        return (zz * NX + xx) * 2 + (core + dc) % 2

    return me, core, lax.axis_index("tp"), there


def meet_all(there, y):
    barrier = pltpu.get_barrier_semaphore()

    def greet(p, carry):
        pl.semaphore_signal(
            barrier, inc=1, device_id={"sp": there(p, 1)}, device_id_type=pl.DeviceIdType.MESH
        )
        return carry

    lax.fori_loop(1, 64, greet, 0)
    for other in ((y + 1) % NY, (y + 3) % NY):
        pl.semaphore_signal(
            barrier, inc=1, device_id={"tp": other}, device_id_type=pl.DeviceIdType.MESH
        )
    return barrier


def swap_matrix():
    r = lax.broadcasted_iota(jnp.int32, (256, 256), 0)
    c = lax.broadcasted_iota(jnp.int32, (256, 256), 1)
    hit = (r // 16 == c % 16) & (r % 16 == c // 16)
    return jnp.where(hit, 1.0, 0.0).astype(jnp.bfloat16)


def to_tiles(swap, rows):
    stacked = jnp.concatenate([rows[:, j * 128 : (j + 1) * 128] for j in range(16)], axis=0)
    return jnp.dot(swap, stacked, preferred_element_type=jnp.float32).astype(jnp.bfloat16)


def from_tiles(swap, tiles, out_ref, first):
    stacked = jnp.dot(swap, tiles, preferred_element_type=jnp.float32).astype(jnp.bfloat16)
    for j in range(16):
        out_ref[pl.ds(first, 16), j * 128 : (j + 1) * 128] = stacked[j * 16 : (j + 1) * 16]


def block(position):
    return pl.ds(pl.multiple_of(position * 48, 16), 48)


def remote(src, dst, send, recv, **where):
    return pltpu.make_async_remote_copy(
        src_ref=src,
        dst_ref=dst,
        send_sem=send,
        recv_sem=recv,
        device_id=where,
        device_id_type=pl.DeviceIdType.MESH,
    )


def experts_kernel(
    out_ref, gate_hbm, up_hbm, down_hbm, back_ref,
    gate, up, down, packed, rows, x_rows, hidden, parts, far, near, both, summed, answers, returned,
    load_sem, send_sem, out_sem, spread_sem, sum_sem, back_sem,
):
    me, core, y, there = places()
    y_up, y_down = (y + 1) % NY, (y + 3) % NY
    ahead, behind = (y + 1 + 2 * core) % NY, (y + 3 - 2 * core) % NY
    to_ahead, to_behind = 3 - 2 * core, 1 + 2 * core
    barrier = meet_all(there, y)
    loads = [
        pltpu.make_async_copy(src, dst, load_sem.at[i])
        for i, (src, dst) in enumerate(((gate_hbm, gate), (up_hbm, up), (down_hbm, down)))
    ]
    for load in loads:
        load.start()
    swap = swap_matrix()

    def tiles_at(first):
        return pl.ds(pl.multiple_of(first, 256), 256)

    def pack(s, carry):
        first = pl.multiple_of(s * 16, 16)
        packed[tiles_at(s * 256), :] = to_tiles(swap, out_ref[pl.ds(first, 16), :])
        return carry

    lax.fori_loop(0, 12, pack, 0)
    rows[0:48, :] = packed[block(me), :]
    pl.semaphore_wait(barrier, 65)

    def hand_out(i, carry):
        p = (i + 16) % 64
        to = there(p, 1)

        @pl.when(p > 0)
        def _():
            remote(
                packed.at[block(to)], rows.at[block(p)], send_sem.at[0], out_sem.at[p], sp=to
            ).start()

        return carry

    lax.fori_loop(0, 64, hand_out, 0)

    def part(relative, k):
        return rows.at[pl.ds(pl.multiple_of(relative * 3072 + k * 768, 256), 768)]

    def along(relative_from, relative_to, k, to):
        return remote(
            part(relative_from, k), part(relative_to, k),
            send_sem.at[1], spread_sem.at[relative_to, k], tp=to,
        )

    def await_row(p, carry):
        remote(
            packed.at[block(p)], rows.at[block(p)], send_sem.at[0], out_sem.at[p], sp=me
        ).wait_recv()
        return carry

    def spread(k):
        lax.fori_loop(jnp.maximum(16 * k, 1), 16 * k + 16, await_row, 0)
        along(0, 1, k, y_up).start()
        along(0, 3, k, y_down).start()

    def pass_on(k):
        along(0, 1, k, y_up).wait_recv()
        along(0, 3, k, y_down).wait_recv()

        @pl.when(core == 0)
        def _():
            along(1, 2, k, y_up).start()

        @pl.when(core == 1)
        def _():
            along(3, 2, k, y_down).start()

    def chunk(k):
        return pl.ds(pl.multiple_of(k * 48, 16), 48)

    def partial(relative, k):
        return pl.ds(pl.multiple_of(k * 192 + relative * 48, 16), 48)

    def send_far(k):
        return remote(
            parts.at[partial(2, k)], far.at[chunk(k)], send_sem.at[2], sum_sem.at[0, k], tp=ahead
        )

    def send_near(k):
        return remote(
            parts.at[partial(to_behind, k)], near.at[chunk(k)],
            send_sem.at[2], sum_sem.at[1, k], tp=behind,
        )

    def send_both(k):
        return remote(
            summed.at[chunk(k)], both.at[chunk(k)], send_sem.at[2], sum_sem.at[2, k], tp=ahead
        )

    def compute(k):
        along(0, 2, k, y_up).wait_recv()

        def unpack_x(i, carry):
            relative, s = i // 3, i % 3
            tiles = rows[tiles_at(relative * 3072 + k * 768 + s * 256), :]
            from_tiles(swap, tiles, x_rows, pl.multiple_of(i * 16, 16))
            return carry

        lax.fori_loop(0, 12, unpack_x, 0)
        mine = x_rows[...]
        for n in range(3):
            columns = slice(n * 256, (n + 1) * 256)
            gated = jnp.dot(mine, gate[:, columns], preferred_element_type=jnp.float32)
            upped = jnp.dot(mine, up[:, columns], preferred_element_type=jnp.float32)
            hidden[:, columns] = (gated / (1.0 + jnp.exp(-gated)) * upped).astype(jnp.bfloat16)
        units = hidden[...]
        for n in range(8):
            columns = slice(n * 256, (n + 1) * 256)
            parts[pl.ds(pl.multiple_of(k * 192, 16), 192), columns] = jnp.dot(
                units, down[:, columns], preferred_element_type=jnp.float32
            ).astype(jnp.bfloat16)
        send_far(k).start()
        send_near(k).start()

    def add_far(k):
        send_far(k).wait_recv()
        summed[chunk(k), :] = (
            parts[partial(to_ahead, k), :].astype(jnp.float32)
            + far[chunk(k), :].astype(jnp.float32)
        ).astype(jnp.bfloat16)
        send_both(k).start()

    def finish(k):
        send_near(k).wait_recv()
        send_both(k).wait_recv()

        def pack_answer(s, carry):
            own = pl.ds(pl.multiple_of(k * 192 + s * 16, 16), 16)
            arrived = pl.ds(pl.multiple_of(k * 48 + s * 16, 16), 16)
            answer = (
                parts[own, :].astype(jnp.float32)
                + near[arrived, :].astype(jnp.float32)
                + both[arrived, :].astype(jnp.float32)
            ).astype(jnp.bfloat16)
            answers[tiles_at(k * 768 + s * 256), :] = to_tiles(swap, answer)
            return carry

        lax.fori_loop(0, 3, pack_answer, 0)

        def give_back(p, carry):
            remote(
                answers.at[block(p)], returned.at[block(me)], send_sem.at[3], back_sem.at[p],
                sp=there(p, -1),
            ).start()
            return carry

        lax.fori_loop(jnp.maximum(16 * k, 1), 16 * k + 16, give_back, 0)

    def tick(t, carry):
        @pl.when(t < 4)
        def _():
            spread((t + 1) % 4)

        @pl.when((t >= 1) & (t < 5))
        def _():
            pass_on(t % 4)

        @pl.when(t == 2)
        def _():
            for load in loads:
                load.wait()

        @pl.when((t >= 2) & (t < 6))
        def _():
            compute((t - 1) % 4)

        @pl.when((t >= 3) & (t < 7))
        def _():
            add_far((t - 2) % 4)

        @pl.when(t >= 4)
        def _():
            finish((t - 3) % 4)

        return carry

    lax.fori_loop(0, 8, tick, 0)
    returned[block(me), :] = answers[0:48, :]

    def await_back(p, carry):
        source = there(p, 1)
        remote(
            answers.at[block(p)], returned.at[block(source)], send_sem.at[3], back_sem.at[p],
            sp=source,
        ).wait_recv()
        return carry

    lax.fori_loop(1, 64, await_back, 0)

    def unpack(s, carry):
        from_tiles(swap, returned[tiles_at(s * 256), :], back_ref, pl.multiple_of(s * 16, 16))
        return carry

    lax.fori_loop(0, 12, unpack, 0)
    for i, sent in enumerate((
        packed.at[pl.ds(0, 63 * 48)],
        rows.at[pl.ds(0, 9216)],
        parts.at[pl.ds(0, 576)],
        answers.at[pl.ds(0, 63 * 48)],
    )):
        pltpu.make_async_copy(sent, sent, send_sem.at[i]).wait()


def expert_layer(outgoing, gate, up, down):
    vmem = pl.BlockSpec(memory_space=pltpu.VMEM)
    hbm = pl.BlockSpec(memory_space=pltpu.HBM)

    def room(*shape):
        return pltpu.VMEM(shape, jnp.bfloat16)

    return pl.pallas_call(
        experts_kernel,
        out_shape=jax.ShapeDtypeStruct((192, 2048), jnp.bfloat16),
        in_specs=[vmem, hbm, hbm, hbm],
        out_specs=vmem,
        scratch_shapes=[
            room(2048, 768), room(2048, 768), room(768, 2048),
            room(3072, 128), room(12288, 128), room(192, 2048), room(192, 768), room(768, 2048),
            room(192, 2048), room(192, 2048), room(192, 2048), room(192, 2048),
            room(3072, 128), room(3072, 128),
            pltpu.SemaphoreType.DMA((3,)),
            pltpu.SemaphoreType.DMA((4,)),
            pltpu.SemaphoreType.DMA((64,)),
            pltpu.SemaphoreType.DMA((NY, 4)),
            pltpu.SemaphoreType.DMA((3, 4)),
            pltpu.SemaphoreType.DMA((64,)),
        ],
        compiler_params=pltpu.CompilerParams(
            collective_id=1, has_side_effects=True, vmem_limit_bytes=56 * 2**20
        ),
        name="experts",
    )(outgoing, gate, up, down)


def local(
    stream_in, queries, keys, values, query_gain, key_gain, out_rows, norm_gain,
    route_ids, route_weights, gate_weight, up_weight, down_weight,
):
    head_size = query_gain.shape[0]
    seq_rows = queries.shape[0]
    cosine, sine = turn_tables(lax.axis_index("sp") * seq_rows, seq_rows, head_size)
    twice = lambda g: jnp.tile(g, 2)[None, :]
    token_heads, whole_out = attention(
        queries, keys, values, twice(query_gain), twice(key_gain), cosine, sine, out_rows
    )
    projected = jnp.dot(token_heads, whole_out, preferred_element_type=jnp.float32)
    stream = (stream_in.astype(jnp.float32) + projected).astype(jnp.bfloat16)
    stream_wide = stream.astype(jnp.float32)
    normed = (
        stream_wide
        * lax.rsqrt(jnp.mean(stream_wide * stream_wide, axis=1, keepdims=True) + EPS)
        * norm_gain
    ).astype(jnp.bfloat16)
    tokens = stream.shape[0]
    model_width = stream.shape[1]
    top_count = route_ids.shape[1]
    experts = lax.axis_size("sp")
    routed = tokens * top_count
    capacity = SLOTS
    flat_ids = route_ids.reshape(routed)
    member = (flat_ids[:, None] == jnp.arange(experts, dtype=jnp.int32)[None, :]).astype(jnp.int32)
    earlier = jnp.cumsum(member, axis=0) - member
    slot_rank = jnp.sum(earlier * member, axis=1)
    target = flat_ids * capacity + slot_rank
    placed = (target[:, None] == jnp.arange(experts * capacity, dtype=jnp.int32)[None, :]).astype(
        jnp.bfloat16
    )
    placed = placed.reshape(tokens, top_count, experts * capacity)
    outgoing = jnp.einsum("tks,td->sd", placed, normed, preferred_element_type=jnp.float32).astype(
        jnp.bfloat16
    )
    expert_back = expert_layer(outgoing, gate_weight[0], up_weight[0], down_weight[0])
    picked = jnp.einsum("tks,sd->tkd", placed, expert_back, preferred_element_type=jnp.float32)
    mixed_out = stream_wide + jnp.sum(route_weights[:, :, None] * picked, axis=1)
    return mixed_out.astype(jnp.bfloat16)


def solution(mesh):
    return jax.shard_map(
        local,
        mesh=mesh,
        in_specs=(
            P(("sp", "tp"), None),
            P("sp", "tp"),
            P("sp", "tp"),
            P("sp", "tp"),
            P(),
            P(),
            P("tp", None),
            P(),
            P(("sp", "tp"), None),
            P(("sp", "tp"), None),
            P("sp", None, "tp"),
            P("sp", None, "tp"),
            P("sp", "tp", None),
        ),
        out_specs=P(("sp", "tp"), None),
        check_vma=False,
    )
```
